32 devices in a mesh: grp: 2 (over y), ep: 8 (over z, core), tp: 2 (over x).
Axes of the slice: x: 2, y: 2, z: 4, core: 2. Of those that a mesh axis runs over, the one named last changes fastest.
Arguments:
- value_in: bfloat16 [8192, 1024], P(('grp', 'ep'), 'tp'), parts along dimension 0, may hold values from -6 to 6
- gate_in: bfloat16 [8192, 1024], P(('grp', 'ep'), 'tp'), parts along dimension 0, may hold values from -6 to 6
- conv_taps: float32 [31, 1024], P(None, 'tp'), may hold values from -12 to 12
- chan_gain: float32 [1024], replicated, may hold values from 0.1 to 1.9
- out_weight: bfloat16 [1024, 2048], P(None, 'tp'), may hold values from -0.1875 to 0.1875
- second_rows: bfloat16 [2048, 2048], P(('grp', 'ep')), parts along dimension 0, may hold values from -6 to 6
- expert_gain: float32 [2048], replicated, may hold values from 0.1 to 1.9
- routes: int32 [2048, 2], P(('grp', 'ep')), parts along dimension 0, may hold values from 0 to 3, all different within a row; in each aligned block of 128 rows (0 to 127, 128 to 255, ...) at most 96 rows name the same one
- route_weights: float32 [2048, 2], P(('grp', 'ep')), parts along dimension 0, may hold values from 0.1 to 0.9
- gate_w: bfloat16 [8, 2048, 2048], P('ep', None, 'tp'), may hold values from -0.125 to 0.125
- up_w: bfloat16 [8, 2048, 2048], P('ep', None, 'tp'), may hold values from -0.125 to 0.125
- down_w: bfloat16 [8, 2048, 2048], P('ep', 'tp'), may hold values from -0.125 to 0.125
Outputs:
- mixer_rows: bfloat16 [8192, 2048], P(('grp', 'ep'), 'tp'), parts along dimension 0
- routed_rows: bfloat16 [2048, 2048], P(('grp', 'ep'), 'tp'), parts along dimension 0
The draws below stay inside these ranges and needn't reach their ends.
There are 2 independent parts, one for each index of `grp`. The reference program is written for one: setup_inputs(seed, part) draws one part's arguments, and reference() takes and returns one part's arrays. A program takes and returns all parts, laid end to end along the dimension named above; an argument that names none is the same for every part. Nothing has to cross between parts.
Inputs may be any that keep to these rules, and one draw needn't show every extreme that they name: `routes`: in each aligned block of 128 rows (the rows of one index of ep) no expert is named by more than 96 rows, a bound that some block reaches; each row names 2 different experts.
All inputs are finite; a program needn't handle non-finite values.
Results may differ from the reference program's by a relative error of at most 0.017.
Values may be sent and summed in bfloat16 or wider, within the bound.
A program may use at most 64 MiB of HBM per device.

```python
import math
import jax
import jax.numpy as jnp
import numpy as np
from jax import lax

D = 2048
CONV_CH = 1024
TAPS = 31
FF_EXPERT = 4096
TOP = 2
TOK_B = 128
HALF_FF = 2048
EXPERTS = 4
CAP = 96
TOKENS_A = 4096
TOKENS_B = 1024
N_EP = 8
N_TP = 2


def draw_conv_taps(key, part):
    channel = jnp.arange(CONV_CH, dtype=jnp.float32)[None, :] / CONV_CH
    rough = jnp.exp(jax.random.uniform(jax.random.fold_in(key, 7), (1, CONV_CH), jnp.float32, -0.5, 0.5))
    base = jnp.clip(jax.random.normal(jax.random.fold_in(key, 5), (TAPS, CONV_CH), jnp.float32), -4.0, 4.0)
    ramp = jnp.exp(jnp.log(3.0) * channel)
    return base * rough * ramp / math.sqrt(TAPS)


def raised(values, stream_key, source, target, shards_of, factor):
    owner, partner = [(jnp.arange(values.shape[position]) // (values.shape[position] // shards_of)).reshape([-1 if axis == position else 1 for axis in range(values.ndim)]) for position in (source, target)]
    chosen = jax.random.permutation(stream_key, shards_of)[partner]
    strong = (owner == chosen) | (owner == (partner + shards_of // 2) % shards_of)
    return jnp.where(strong, factor * values, values)


def level_of(own_key, dims, split, least, high):
    gain, own = 1.0, jax.random.fold_in(own_key, 6)
    for dim, blocks in split:
        heights = jnp.exp(jax.random.uniform(jax.random.fold_in(own, dim), (blocks,), jnp.float32, least / len(split), high / len(split)))
        gain = gain * jnp.repeat(heights, dims[dim] // blocks).reshape([-1 if axis == dim else 1 for axis in range(len(dims))])
    return gain


def shared_out(key, own, number, rows, number_of, top, reach, skew):
    order = jax.random.permutation(key, number_of)
    heavy_load, usual = load_shares(number_of, rows * top, reach, skew, True), load_shares(number_of, rows * top, reach, skew, False)
    places = jnp.arange(number_of)

    def named(sizes, turn):
        used = int((sizes > 0).sum())
        fixed = max(1, used // 4)
        shifted = fixed + (places - fixed + turn * (used - fixed)) % max(1, number_of - fixed)
        return jnp.zeros((number_of,), jnp.int32).at[order[jnp.where(places < fixed, places, shifted)]].set(jnp.asarray(sizes, jnp.int32))

    sizes = jnp.where(number % 4 == 0, named(heavy_load, number // 4), named(usual, number - number // 4 - 1))
    mixed = jax.random.permutation(jax.random.fold_in(own, 3), number_of)
    donor, taker = mixed[0:number_of // 2 * 2:2], mixed[1:number_of // 2 * 2:2]
    slack = jnp.minimum(sizes[donor] - 1, reach - sizes[taker]) // 2
    slack = jnp.where((donor == order[0]) | (taker == order[0]) | (sizes[taker] == 0), 0, jnp.maximum(slack, 0))
    shifted = jax.random.randint(jax.random.fold_in(own, 4), (number_of // 2,), 0, 1 << 20) % (slack + 1)
    sizes = sizes.at[donor].add(-shifted).at[taker].add(shifted)
    members = jnp.searchsorted(jnp.cumsum(sizes), jnp.arange(rows * top), side="right").astype(jnp.int32)
    table = members.reshape(top, rows).T
    table = table[jax.random.permutation(jax.random.fold_in(own, 1), rows)]
    turn = jax.random.randint(jax.random.fold_in(own, 2), (rows, 1), 0, top)
    return jnp.take_along_axis(table, (jnp.arange(top)[None, :] + turn) % top, axis=1)


def load_shares(amount, total, bound, skew, full):
    loads = [(1 << 20) // math.isqrt(rank ** skew) + 1 for rank in range(1, amount + 1)]
    largest = bound if full else min(bound, max(-(-total // amount), total * loads[0] // sum(loads)))
    least = 1 if total - largest >= amount - 1 else 0
    holding, surplus = [largest] + [least] * (amount - 1), total - largest - least * (amount - 1)
    while surplus > 0:
        candidates = [i for i in range(1, amount) if holding[i] < largest] or [i for i in range(1, amount) if holding[i] < bound]
        whole, left = sum([loads[i] for i in candidates]), surplus
        for i in candidates:
            more = min(bound - holding[i], max(1, left * loads[i] // whole), surplus)
            holding[i] = holding[i] + more
            surplus = surplus - more
    return np.array(holding)


def noise(stream_key, extent, deviation, limit, split=(), kind=jnp.bfloat16):
    values = jax.random.normal(stream_key, extent, jnp.float32) * deviation
    if len(split) > 0:
        values = level_of(stream_key, extent, split, -0.22, 0.18) * values
    return jnp.clip(values, min=-limit, max=limit).astype(kind)


def heavy_noise(own_key, shape, spread, most, pieces, heavy, held_as=jnp.bfloat16):
    entries = spread * jax.random.normal(own_key, shape, jnp.float32)
    if pieces:
        entries = entries * level_of(own_key, shape, pieces, -0.22, 0.18)
    return jnp.clip(raised(entries, jax.random.fold_in(own_key, 3), *heavy), -most, most).astype(held_as)


def setup_inputs(seed: int = 0, part: int = 0) -> dict:
    key_list = jax.random.split(jax.random.key(seed), 13)
    part_keys = jax.random.split(jax.random.fold_in(key_list[12], part), 13)
    value_in = noise(part_keys[0], (TOKENS_A, CONV_CH), 1.0, 6.0, ((0, 8), (1, 2)))
    gate_in = noise(part_keys[1], (TOKENS_A, CONV_CH), 1.0, 6.0, ((0, 8), (1, 2)))
    conv_taps = draw_conv_taps(jax.random.fold_in(key_list[12], 71), part)
    chan_gain = jnp.clip(1.0 + 0.18 * jax.random.normal(key_list[3], (CONV_CH,), jnp.float32), 0.1, 1.9)
    out_weight = noise(key_list[4], (CONV_CH, D), CONV_CH ** -0.5, 0.1875, ((1, 2),))
    second_rows = noise(part_keys[5], (TOKENS_B, D), 1.0, 6.0, ((0, 8),))
    expert_gain = jnp.clip(1.0 + 0.18 * jax.random.normal(key_list[6], (D,), jnp.float32), 0.1, 1.9)
    routes_keys = jax.random.split(jax.random.fold_in(part_keys[7], 1), TOKENS_B // TOK_B)
    routes_turns = jax.random.permutation(jax.random.fold_in(part_keys[7], 3), TOKENS_B // TOK_B)
    routes = jax.vmap(lambda own, number: shared_out(jax.random.fold_in(part_keys[7], 2), own, number, TOK_B, EXPERTS, TOP, CAP, 1))(routes_keys, routes_turns).reshape((TOKENS_B, TOP))
    route_weights = jnp.clip(0.1 + 0.79999997 * jax.random.uniform(part_keys[8], (TOKENS_B, TOP), jnp.float32) ** level_of(part_keys[8], (TOKENS_B, TOP), ((0, 8),), -0.2, 0.2), 0.1, 0.9)
    gate_w = noise(key_list[9], (2 * EXPERTS, D, HALF_FF), D ** -0.5, 0.125, ((0, 8), (2, 2)))
    up_w = noise(key_list[10], (2 * EXPERTS, D, HALF_FF), D ** -0.5, 0.125, ((0, 8), (2, 2)))
    down_w = heavy_noise(key_list[11], (2 * EXPERTS, HALF_FF, D), FF_EXPERT ** -0.5, 0.125, ((0, 8), (1, 2)), (1, 2, 2, 2.0))
    return dict(value_in=value_in, gate_in=gate_in, conv_taps=conv_taps, chan_gain=chan_gain, out_weight=out_weight, second_rows=second_rows, expert_gain=expert_gain, routes=routes, route_weights=route_weights, gate_w=gate_w, up_w=up_w, down_w=down_w)


eps = 1e-06

def expert_values(rows, gate_pair, up_pair, down_pair):
    halves = []
    for half in range(2):
        gate = jnp.dot(rows, gate_pair[half], preferred_element_type=jnp.float32)
        upper = jnp.dot(rows, up_pair[half], preferred_element_type=jnp.float32)
        hidden = (jax.nn.silu(gate) * upper).astype(jnp.bfloat16)
        block = hidden.shape[1] // N_TP
        total = jnp.zeros((rows.shape[0], down_pair.shape[2]), jnp.float32)
        for index in range(N_TP):
            piece = jnp.dot(hidden[:, index * block:(index + 1) * block], down_pair[half, index * block:(index + 1) * block], preferred_element_type=jnp.float32)
            total = total + lax.optimization_barrier(piece.astype(jnp.bfloat16)).astype(jnp.float32)
        halves.append(lax.optimization_barrier(total.astype(jnp.bfloat16)).astype(jnp.float32))
    return (halves[0] + halves[1]).astype(jnp.bfloat16)

def reference(value_in, gate_in, conv_taps, chan_gain, out_weight, second_rows, expert_gain, routes, route_weights, gate_w, up_w, down_w):
    glu = (value_in.astype(jnp.float32) * jax.nn.sigmoid(gate_in.astype(jnp.float32))).astype(jnp.bfloat16)
    length = glu.shape[0]
    padded = jnp.concatenate([jnp.zeros((TAPS - 1, glu.shape[1]), jnp.float32), glu.astype(jnp.float32)], axis=0)
    total = jnp.zeros(glu.shape, jnp.float32)
    for offset in range(TAPS):
        total = total + conv_taps[offset][None, :] * padded[offset:offset + length]
    values = total.astype(jnp.bfloat16).astype(jnp.float32)
    centered = values - lax.optimization_barrier(jnp.mean(values, axis=-1, keepdims=True))
    scaled = centered * lax.rsqrt(lax.optimization_barrier(jnp.mean(centered * centered, axis=-1, keepdims=True)) + eps) * chan_gain
    activated = jax.nn.silu(scaled).astype(jnp.bfloat16)
    mixer_rows = jnp.dot(activated, out_weight, preferred_element_type=jnp.float32).astype(jnp.bfloat16)
    rows = second_rows.astype(jnp.float32)
    normed = (rows * lax.rsqrt(lax.optimization_barrier(jnp.mean(rows * rows, axis=-1, keepdims=True)) + eps) * expert_gain).astype(jnp.bfloat16)
    tokens = normed.shape[0]
    chosen = routes.reshape(-1).astype(jnp.int32)
    hits = (chosen[:, None] == jnp.arange(EXPERTS, dtype=jnp.int32)[None, :]).astype(jnp.int32)
    place = lax.optimization_barrier(jnp.sum((jnp.cumsum(hits, axis=0) - 1) * hits, axis=1)).astype(jnp.int32)
    owner = jnp.repeat(jnp.arange(tokens, dtype=jnp.int32), TOP)
    span = N_EP * CAP
    table = jnp.full((EXPERTS, span), tokens, jnp.int32).at[chosen, place].set(owner)
    padded_rows = jnp.concatenate([normed, jnp.zeros((1, normed.shape[1]), jnp.bfloat16)], axis=0)
    gate_pairs = gate_w.reshape(EXPERTS, 2, gate_w.shape[1], gate_w.shape[2])
    up_pairs = up_w.reshape(EXPERTS, 2, up_w.shape[1], up_w.shape[2])
    down_pairs = down_w.reshape(EXPERTS, 2, down_w.shape[1], down_w.shape[2])

    def one_expert(packed):
        index, gate_pair, up_pair, down_pair = packed
        return expert_values(padded_rows[index], gate_pair, up_pair, down_pair)
    outputs = lax.map(one_expert, (table, gate_pairs, up_pairs, down_pairs))
    flat = outputs.reshape(EXPERTS * span, outputs.shape[2])
    picked = flat[(chosen * span + place).astype(jnp.int32)].astype(jnp.float32)
    weighted = picked * route_weights.reshape(-1)[:, None]
    routed_rows = lax.optimization_barrier(jnp.sum(weighted.reshape(tokens, TOP, weighted.shape[1]), axis=1)).astype(jnp.bfloat16)
    return (mixer_rows, routed_rows)
```

```python
import functools

import jax
import jax.numpy as jnp
from jax import lax
from jax.experimental import pallas as pl
from jax.experimental.pallas import tpu as pltpu
from jax.sharding import PartitionSpec as P

eps = 1e-06
LANES = 128
MESH = pl.DeviceIdType.MESH


def partner_2(value, axis, bit):
    return lax.ppermute(value, axis, [(i, i ^ 1 << bit) for i in range(lax.axis_size(axis))])


def shifted(value, axis, by):
    devices = lax.axis_size(axis)
    pairs = [(i, i + by) for i in range(devices) if 0 <= i + by < devices]
    return lax.ppermute(value, axis, pairs)


def partner(block):
    return partner_2(block, "ep", 0)


def across(block):
    return lax.all_to_all(block, "ep", split_axis=0, concat_axis=0, tiled=True)


def on_device(
    value_in,
    gate_in,
    conv_taps,
    chan_gain,
    out_weight,
    second_rows,
    expert_gain,
    routes,
    route_weights,
    gate_w,
    up_w,
    down_w,
):
    taps = conv_taps.shape[0]
    glu = (value_in.astype(jnp.float32) * jax.nn.sigmoid(gate_in.astype(jnp.float32))).astype(
        jnp.bfloat16
    )
    length = glu.shape[0]
    before = shifted(glu[length - taps + 1 :], "ep", 1)
    padded = jnp.concatenate([before, glu], axis=0).astype(jnp.float32)
    total = jnp.zeros(glu.shape, jnp.float32)
    for offset in range(taps):
        total = total + conv_taps[offset][None, :] * padded[offset : offset + length]
    convolved = total.astype(jnp.bfloat16)
    channels = lax.all_gather(convolved, "tp", axis=1, tiled=True)
    values = channels.astype(jnp.float32)
    centered = values - jnp.mean(values, axis=-1, keepdims=True)
    scaled = (
        centered
        * lax.rsqrt(jnp.mean(centered * centered, axis=-1, keepdims=True) + eps)
        * chan_gain
    )
    activated = jax.nn.silu(scaled).astype(jnp.bfloat16)
    mixer_rows = jnp.dot(activated, out_weight, preferred_element_type=jnp.float32).astype(
        jnp.bfloat16
    )
    n_ep = lax.axis_size("ep")
    experts = n_ep // 2
    tokens = second_rows.shape[0]
    top = routes.shape[1]
    width = second_rows.shape[1]
    capacity = 2 * max(1, min(tokens // 2, 3 * tokens * top // (4 * experts)))
    half_slots = capacity // 2
    rows = second_rows.astype(jnp.float32)
    normed = (
        rows * lax.rsqrt(jnp.mean(rows * rows, axis=-1, keepdims=True) + eps) * expert_gain
    ).astype(jnp.bfloat16)
    chosen = routes.reshape(-1)
    hits = (chosen[:, None] == jnp.arange(experts, dtype=jnp.int32)[None, :]).astype(jnp.int32)
    place = jnp.sum((jnp.cumsum(hits, axis=0) - 1) * hits, axis=1)
    target = (chosen * capacity + place).reshape(tokens, top)
    slots = jnp.arange(experts * capacity, dtype=jnp.int32)
    matches = target[:, :, None] == slots[None, None, :]
    picker = jnp.any(matches, axis=1).astype(jnp.bfloat16)
    outgoing = jnp.dot(picker.T, normed, preferred_element_type=jnp.float32).astype(jnp.bfloat16)
    combiner = jnp.sum(jnp.where(matches, route_weights[:, :, None], 0.0), axis=1)
    upper = lax.axis_index("ep") % 2
    arrived = across(outgoing.reshape(n_ep, half_slots, width))
    other = partner(arrived)
    first = jnp.where(upper == 0, arrived, other)
    second = jnp.where(upper == 0, other, arrived)
    incoming = jnp.concatenate([first, second], axis=1)
    block_rows = incoming.reshape(n_ep * capacity, width)
    gate = jnp.dot(block_rows, gate_w[0], preferred_element_type=jnp.float32)
    lifted = jnp.dot(block_rows, up_w[0], preferred_element_type=jnp.float32)
    hidden = (jax.nn.silu(gate) * lifted).astype(jnp.bfloat16)
    partial_value = jnp.dot(hidden, down_w[0], preferred_element_type=jnp.float32)
    half_sums = lax.psum_scatter(
        partial_value.astype(jnp.bfloat16), "tp", scatter_dimension=1, tiled=True
    )
    columns = half_sums.shape[1]
    half_sums = half_sums.reshape(n_ep, capacity, columns)
    other_sums = partner(half_sums)
    joined = (half_sums.astype(jnp.float32) + other_sums.astype(jnp.float32)).astype(jnp.bfloat16)
    own = lax.dynamic_slice_in_dim(joined, upper * half_slots, half_slots, 1)
    results = across(own).reshape(experts * capacity, columns)
    routed_rows = jnp.dot(
        combiner,
        results.astype(jnp.float32),
        precision=lax.Precision.HIGHEST,
        preferred_element_type=jnp.float32,
    ).astype(jnp.bfloat16)
    return (mixer_rows, routed_rows)


def _xor(value, mask):
    out, bit = value, 1
    while bit <= mask:
        if mask & bit:
            out = out + bit - 2 * bit * lax.rem(lax.div(value, bit), 2)
        bit *= 2
    return out


def _iota(shape, dim):
    return lax.broadcasted_iota(jnp.int32, shape, dim)


def _dot(a, b):
    return jnp.dot(a, b, preferred_element_type=jnp.float32)


def step_kernel(
    chips,
    cap,
    subs,
    pieces,
    halo,
    value_hbm,
    gate_hbm,
    taps_hbm,
    gain_hbm,
    wo_hbm,
    rows_hbm,
    egain_hbm,
    routes_hbm,
    rw_hbm,
    wg_hbm,
    wu_hbm,
    wd_hbm,
    mixer_ref,
    routed_ref,
    value_ref,
    gate_ref,
    taps_ref,
    gain_ref,
    rows_ref,
    egain_ref,
    routes_t_ref,
    rw_t_ref,
    wo,
    wg,
    wu,
    wd,
    normed,
    picked,
    block,
    hid,
    part,
    pair_in,
    cross_out,
    cross_in,
    back_out,
    results,
    near_out,
    near_res,
    q_out,
    q_in,
    combs,
    acc,
    glu,
    halo_out,
    halo_in,
    conv,
    w_sem,
    in_sem,
    disp_send,
    disp_recv,
    xf_send,
    xf_recv,
    cf_send,
    cf_recv,
    r1_send,
    r1_recv,
    r2_send,
    r2_recv,
    r3_send,
    r3_recv,
    r4_send,
    r4_recv,
    q_send,
    q_recv,
    ag_send,
    ag_recv,
    halo_send,
    halo_recv,
):
    f32, bf16 = jnp.float32, jnp.bfloat16
    ep = lax.axis_index("ep")
    x = lax.axis_index("tp")
    n_ep = 2 * chips
    z, c = lax.div(ep, 2), lax.rem(ep, 2)
    width = block.shape[-1]
    tokens = rows_ref.shape[0]
    length, local = value_ref.shape
    cols = local // LANES
    ntaps = taps_ref.shape[0]
    few = cap // subs
    split_from = max(1, chips // 2)
    far = list(range(split_from, chips))
    near = list(range(1, split_from))
    swap = 1 - lax.rem(z + lax.div(z, 2), 2)
    peers = [_xor(z, k) for k in range(chips)]
    for k in far:
        peers[k] = peers[k] + swap * (1 - 2 * lax.rem(peers[k], 2))

    def dev(zd, cd, xd):
        return {"ep": zd * 2 + cd, "tp": xd}

    def remote(src, dst, send, recv, to):
        return pltpu.make_async_remote_copy(
            src_ref=src, dst_ref=dst, send_sem=send, recv_sem=recv, device_id=to, device_id_type=MESH
        )

    core_peer = dev(z, 1 - c, x)
    plane_peer = dev(z, c, 1 - x)
    after = {"ep": lax.rem(ep + 1, n_ep), "tp": x}
    prior = {"ep": lax.rem(ep + n_ep - 1, n_ep), "tp": x}
    sends = []

    def start(copy):
        copy.start()
        sends.append(copy)

    barrier = pltpu.get_barrier_semaphore()
    greeted = [core_peer, plane_peer, after, prior] + [dev(peers[k], c, x) for k in range(1, chips)]
    for to in greeted:
        pl.semaphore_signal(barrier, inc=1, device_id=to, device_id_type=MESH)

    inputs = [
        (rows_hbm, rows_ref),
        (routes_hbm, routes_t_ref),
        (rw_hbm, rw_t_ref),
        (egain_hbm, egain_ref),
        (value_hbm, value_ref),
        (gate_hbm, gate_ref),
        (taps_hbm, taps_ref),
        (gain_hbm, gain_ref),
    ]
    inputs = [pltpu.make_async_copy(a, b, in_sem.at[i]) for i, (a, b) in enumerate(inputs)]
    weights = [
        pltpu.make_async_copy(wg_hbm.at[0], wg, w_sem.at[0]),
        pltpu.make_async_copy(wu_hbm.at[0], wu, w_sem.at[1]),
        pltpu.make_async_copy(wd_hbm.at[0], wd, w_sem.at[2]),
        pltpu.make_async_copy(wo_hbm, wo, w_sem.at[3]),
    ]
    for copy in inputs:
        copy.start()
    for copy in inputs[:4]:
        copy.wait()
    erows = -(-chips // 8) * 8
    r0t, r1t = routes_t_ref[0:1, :], routes_t_ref[1:2, :]
    eid = _iota((erows, tokens), 0)
    hits_t = (r0t == eid) | (r1t == eid)
    earlier_t = (_iota((tokens, tokens), 0) < _iota((tokens, tokens), 1)).astype(f32)
    place_t = _dot(hits_t.astype(f32).astype(bf16), earlier_t.astype(bf16))
    slot_t = jnp.where(hits_t, place_t, -1.0).astype(jnp.int32)

    rows = rows_ref[...].astype(f32)
    scale = lax.rsqrt(jnp.mean(rows * rows, axis=-1, keepdims=True) + eps)
    both = (rows * scale * egain_ref[...]).astype(bf16)
    normed[0] = both[:, :width]
    normed[1] = both[:, width:]

    slots = _iota((cap, tokens), 0)

    def pick(k):
        row = jnp.sum(jnp.where(eid == peers[k], slot_t, 0), axis=0, keepdims=True)
        return (slots == row).astype(f32).astype(bf16)

    def cut(s):
        return slice(s * few, (s + 1) * few)

    for k in far:
        rows_k = _dot(pick(k), normed[x]).astype(bf16)
        for s in range(subs):
            picked[k, 0, s] = rows_k[cut(s)]
    for copy in inputs[4:]:
        copy.wait()
    for copy in weights:
        copy.start()
    last = slice(length - halo, length)
    gated = value_ref[last, :].astype(f32) * jax.nn.sigmoid(gate_ref[last, :].astype(f32))
    halo_out[...] = gated.astype(bf16)

    pl.semaphore_wait(barrier, len(greeted))
    halo_copy = remote(halo_out, halo_in, halo_send.at[0], halo_recv.at[0], after)
    start(halo_copy)

    def dispatch(k, h, s, slot):
        start(
            remote(
                picked.at[k, slot, s],
                block.at[z, h, s, c],
                disp_send.at[k, slot, s],
                disp_recv.at[z, slot, s],
                dev(peers[k], c, x),
            )
        )

    def arrived(k, h, s, slot):
        here = block.at[peers[k], h, s, c]
        remote(
            here, here, disp_send.at[k, slot, s], disp_recv.at[peers[k], slot, s], dev(peers[k], c, x)
        ).wait_recv()

    def to_core(k, h, s):
        here = block.at[peers[k], h, s, c]
        start(remote(here, here, cf_send.at[k, h, s], cf_recv.at[k, h, s], core_peer))

    def from_core(k, h, s):
        here = block.at[peers[k], h, s, 1 - c]
        remote(here, here, cf_send.at[k, h, s], cf_recv.at[k, h, s], core_peer).wait_recv()

    def plane_copy(k, h, s):
        here = block.at[peers[k], h, s, c]
        return remote(here, here, xf_send.at[k, s], xf_recv.at[k, s], plane_peer)

    def pair_copy(k, o, s, n):
        h = x if o else 1 - x
        span = pl.ds(s * few, n)
        return remote(
            part.at[k, 1 - c, h, span],
            pair_in.at[k, h, span],
            r1_send.at[k, o, s],
            r1_recv.at[k, o, s],
            core_peer,
        )

    def cross_copy(k, s, n):
        span = pl.ds(s * few, n)
        return remote(
            cross_out.at[k, span], cross_in.at[k, span], r2_send.at[k, s], r2_recv.at[k, s], plane_peer
        )

    def back_copy(k, s, n, at):
        span = pl.ds(s * few, n)
        return remote(
            back_out.at[k, span],
            results.at[at, span],
            r3_send.at[k, s],
            r3_recv.at[at, s],
            dev(peers[k], c, x),
        )

    def feed_forward(k, s, n, between=None, after_half=None):
        count = n // few
        zs = peers[k]
        a0 = block[zs, 0, s : s + count].reshape(2 * n, width)
        a1 = block[zs, 1, s : s + count].reshape(2 * n, width)
        units = hid.shape[1]
        step = min(units, 256)
        for j in range(0, units, step):
            gate = _dot(a0, wg[:width, j : j + step]) + _dot(a1, wg[width:, j : j + step])
            up = _dot(a0, wu[:width, j : j + step]) + _dot(a1, wu[width:, j : j + step])
            hid[: 2 * n, j : j + step] = (gate * jax.nn.sigmoid(gate) * up).astype(bf16)
        if between:
            between()
        h_all = hid[: 2 * n, :]
        for o in range(2):
            if o and after_half:
                after_half()
            h = x if o else 1 - x
            for j in range(0, width, step):
                at = pl.ds(pl.multiple_of(h * width + j, step), step)
                out = _dot(h_all, wd[:, at]).astype(bf16)
                for i in range(count):
                    for core in range(2):
                        r = (2 * i + core) * few
                        part[k, core, h, cut(s + i), j : j + step] = out[r : r + few]
            start(pair_copy(k, o, s, n))

    def pair_sum(k, s, n, wait=True):
        if wait:
            pair_copy(k, 0, s, n).wait_recv()
        span = slice(s * few, s * few + n)
        total = part[k, c, 1 - x, span].astype(f32) + pair_in[k, 1 - x, span].astype(f32)
        cross_out[k, span] = total.astype(bf16)
        start(cross_copy(k, s, n))

    def plane_sum(k, s, n, wait=True):
        if wait:
            pair_copy(k, 1, s, n).wait_recv()
        cross_copy(k, s, n).wait_recv()
        span = slice(s * few, s * few + n)
        total = (
            part[k, c, x, span].astype(f32)
            + pair_in[k, x, span].astype(f32)
            + cross_in[k, span].astype(f32)
        )
        back_out[k, span] = total.astype(bf16)
        start(back_copy(k, s, n, z))

    def near_copy(k, o):
        return remote(
            near_out.at[k, o], near_res.at[k, o], r4_send.at[k, o], r4_recv.at[k, o], dev(peers[k], c, x)
        )

    def near_sum(k, o):
        pair_copy(k, o, 0, cap).wait_recv()
        h = x if o else 1 - x
        total = part[k, c, h].astype(f32) + pair_in[k, h].astype(f32)
        near_out[k, o] = total.astype(bf16)
        if k:
            start(near_copy(k, o))

    q_copy = remote(q_out, q_in, q_send.at[0], q_recv.at[0], plane_peer)

    def close(o):
        total = weighed(0, near_out[0, o])
        for k in near:
            near_copy(k, o).wait_recv()
            total = total + weighed(k, near_res[k, o])
        if o:
            acc[...] = total
        else:
            q_out[...] = total.astype(bf16)
            start(q_copy)

    def pair_sums(k):
        pair_copy(k, 0, 0, cap).wait_recv()
        for s in range(subs):
            pair_sum(k, s, few, False)

    def plane_sums(k):
        pair_copy(k, 1, 0, cap).wait_recv()
        for s in range(subs):
            plane_sum(k, s, few, False)

    def send_far():
        for s in range(subs):
            for k in far:
                dispatch(k, x, s, 0)

    def far_in(k, s):
        arrived(k, x, s, 0)
        start(plane_copy(k, x, s))
        to_core(k, x, s)

    def far_over(k, s):
        plane_copy(k, 1 - x, s).wait_recv()
        to_core(k, 1 - x, s)

    def far_experts(k, s):
        for h in range(2):
            from_core(k, h, s)
        feed_forward(k, s, few)

    def near_in(k):
        for h in range(2):
            for s in range(subs):
                arrived(k, h, s, h)
                to_core(k, h, s)

    def from_cores(k):
        for h in range(2):
            for s in range(subs):
                from_core(k, h, s)

    def weighed(k, found):
        return _dot(combs[k, 0], found) + _dot(combs[k, 1], found)

    rows_per = length // pieces
    tile = 64 if rows_per % 64 == 0 else rows_per

    def gather_copy(p, who):
        rows_p = conv.at[who, pl.ds(p * rows_per, rows_per)]
        return remote(rows_p, rows_p, ag_send.at[p], ag_recv.at[p], plane_peer)

    def gather(lo, hi):
        for p in range(lo, hi):
            start(gather_copy(p, x))

    def convolve(lo, hi, send=False):
        def conv_tile(r, carry):
            r0 = pl.multiple_of(r * tile, tile)
            for i in range(cols):
                total = jnp.zeros((tile, LANES), f32)
                for k in range(ntaps):
                    total = (
                        total
                        + taps_ref[k : k + 1, i * LANES : (i + 1) * LANES]
                        * glu[i, pl.ds(r0 + (k + halo - ntaps + 1), tile), :]
                    )
                conv[x, pl.ds(r0, tile), i * LANES : (i + 1) * LANES] = total.astype(bf16)
            if send:
                gather_copy(r, x).start()
            return carry

        per = rows_per // tile
        send = send and per == 1
        lax.fori_loop(lo * per, hi * per, conv_tile, 0)
        if send:
            sends.extend(gather_copy(p, x) for p in range(lo, hi))
        return send

    def mix(lo, hi):
        for p in range(lo, hi):
            gather_copy(p, 1 - x).wait_recv()
        here = slice(lo * rows_per, hi * rows_per)
        first, second = conv[0, here, :].astype(f32), conv[1, here, :].astype(f32)
        count = 2 * local
        mean = (
            jnp.sum(first, axis=-1, keepdims=True) + jnp.sum(second, axis=-1, keepdims=True)
        ) / count
        first, second = first - mean, second - mean
        var = (
            jnp.sum(first * first, axis=-1, keepdims=True)
            + jnp.sum(second * second, axis=-1, keepdims=True)
        ) / count
        scale = lax.rsqrt(var + eps)
        first = first * scale * gain_ref[:, :local]
        second = second * scale * gain_ref[:, local:]
        first = (first * jax.nn.sigmoid(first)).astype(bf16)
        second = (second * jax.nn.sigmoid(second)).astype(bf16)
        mixer_ref[here, :] = (_dot(first, wo[:local, :]) + _dot(second, wo[local:, :])).astype(bf16)

    def combine(k):
        return acc[...] + weighed(k, results[peers[k]])

    def returned(k, n):
        for s in range(0, cap // few, n // few):
            zs = peers[k]
            span = pl.ds(s * few, n)
            remote(
                back_out.at[k, span],
                results.at[zs, span],
                r3_send.at[k, s],
                r3_recv.at[zs, s],
                dev(zs, c, x),
            ).wait_recv()

    send_far()
    for k in near:
        rows_k = [_dot(pick(k), normed[h]).astype(bf16) for h in range(2)]
        for h in range(2):
            for s in range(subs):
                picked[k, h, s] = rows_k[h][cut(s)]
                dispatch(k, h, s, h)
    for h in range(2):
        rows_0 = _dot(pick(0), normed[h]).astype(bf16)
        for s in range(subs):
            block[z, h, s, c] = rows_0[cut(s)]
    for h in range(2):
        for s in range(subs):
            to_core(0, h, s)
    kept = slice(0, length - halo)
    for i in range(cols):
        at = slice(i * LANES, (i + 1) * LANES)
        gated = value_ref[kept, at].astype(f32) * jax.nn.sigmoid(gate_ref[kept, at].astype(f32))
        glu[i, halo:length, :] = gated.astype(bf16).astype(f32)
        glu[i, length:, :] = halo_out[:, at].astype(f32)
    early = min(pieces, 4)
    if not convolve(1, early, True):
        gather(1, early)
    convolve(early, pieces)
    mid_far, last_far = far[:-1], far[-1]
    units = [(k, s) for k in mid_far for s in range(subs)]
    for copy in weights[:3]:
        copy.wait()
    from_cores(0)
    feed_forward(0, 0, cap, lambda: far_in(*units[0]))
    halo_copy.wait_recv()
    before = jnp.where(ep > 0, halo_in[...].astype(f32), 0.0)
    for i in range(cols):
        glu[i, :halo, :] = before[:, i * LANES : (i + 1) * LANES]
    convolve(0, 1)
    lane = _iota((tokens, LANES), 1)
    index = _iota((8, tokens), 0)
    rows_named = jnp.where(index == 0, r0t, 0).astype(f32) + jnp.where(index == 1, r1t, 0).astype(f32)
    for j in range(2):
        rows_named = rows_named + jnp.where(index == 2 + j, rw_t_ref[j : j + 1, :], 0.0)
    named = jnp.transpose(rows_named)
    r0, r1 = (named[:, j : j + 1].astype(jnp.int32) for j in range(2))
    hits = ((r0 == lane) | (r1 == lane)).astype(f32).astype(bf16)
    earlier = (_iota((tokens, tokens), 1) < _iota((tokens, tokens), 0)).astype(f32).astype(bf16)
    place = _dot(earlier, hits)
    slot_of = _iota((tokens, cap), 1)
    places = [
        jnp.sum(jnp.where(lane == r, place, 0.0), axis=1, keepdims=True).astype(jnp.int32)
        for r in (r0, r1)
    ]
    for k in range(chips):
        comb = jnp.zeros((tokens, cap), f32)
        for j, r in enumerate((r0, r1)):
            mine = jnp.where(r == peers[k], places[j], -1)
            comb = comb + jnp.where(slot_of == mine, named[:, 2 + j : 3 + j], 0.0)
        head = comb.astype(bf16)
        combs[k, 0] = head
        combs[k, 1] = (comb - head.astype(f32)).astype(bf16)


    far_over(*units[0])
    for unit in units[1:]:
        far_in(*unit)
    later = min(pieces, early + 2)
    gather(early, later)
    for o in range(2):
        near_sum(0, o)
    for h in range(2):
        from_core(units[0][0], h, units[0][1])
    feed_forward(*units[0], few)
    for i in range(1, len(units)):
        far_over(*units[i])
        pair_sum(*units[i - 1], few)
        for h in range(2):
            from_core(units[i][0], h, units[i][1])
        feed_forward(*units[i], few, (lambda: far_in(last_far, 0)) if i == 1 else None)
    if len(units) == 1:
        far_in(last_far, 0)
    for k in near:
        near_in(k)
    pair_sum(*units[-1], few)
    far_over(last_far, 0)
    for s in range(1, subs):
        far_in(last_far, s)
    gather(later, pieces)
    gather(0, 1)
    for k in near:
        from_cores(k)
    for k in near:
        feed_forward(k, 0, cap, (lambda: plane_sum(*units[0], few)) if k == near[0] else None)
    for k in near:
        near_sum(k, 0)
    for s in range(1, subs):
        far_over(last_far, s)
    for k in near:
        near_sum(k, 1)
    for unit in units[1:]:
        plane_sum(*unit, few)
    from_cores(last_far)
    feed_forward(last_far, 0, cap)
    pair_sums(last_far)
    weights[3].wait()
    group = 2 if pieces % 2 == 0 else 1
    half = pieces // 2 // group * group
    for p in range(group, half, group):
        mix(p, p + group)
    close(0)
    plane_sums(last_far)
    close(1)
    for p in range(max(half, group), pieces, group):
        mix(p, p + group)
    mix(0, group)
    for k in far[:-1]:
        returned(k, few)
        acc[...] = combine(k)
    q_copy.wait_recv()
    acc[...] = acc[...] + q_in[...].astype(f32)
    returned(far[-1], few)
    routed_ref[...] = combine(far[-1]).astype(bf16)

    for copy in sends:
        copy.wait_send()


def one_kernel(
    value_in,
    gate_in,
    conv_taps,
    chan_gain,
    out_weight,
    second_rows,
    expert_gain,
    routes,
    route_weights,
    gate_w,
    up_w,
    down_w,
):
    chips = lax.axis_size("ep") // 2
    tokens, model = second_rows.shape
    top = routes.shape[1]
    width = model // 2
    cap = 2 * max(1, min(tokens // 2, 3 * tokens * top // (4 * chips)))
    subs = 2 if cap % 32 == 0 else 1
    few = cap // subs
    length, local = value_in.shape
    units = gate_w.shape[2]
    halo = -(-(conv_taps.shape[0] - 1) // 16) * 16
    pieces = 8 if length % 128 == 0 and length // 8 > halo else 1
    bf16, f32 = jnp.bfloat16, jnp.float32
    vmem = pl.BlockSpec(memory_space=pltpu.VMEM)
    hbm = pl.BlockSpec(memory_space=pltpu.HBM)
    dma = pltpu.SemaphoreType.DMA
    scratch = [
        pltpu.VMEM(value_in.shape, bf16),
        pltpu.VMEM(gate_in.shape, bf16),
        pltpu.VMEM(conv_taps.shape, f32),
        pltpu.VMEM((1, chan_gain.shape[0]), f32),
        pltpu.VMEM(second_rows.shape, bf16),
        pltpu.VMEM((1, model), f32),
        pltpu.VMEM((top, tokens), jnp.int32),
        pltpu.VMEM((top, tokens), f32),
        pltpu.VMEM(out_weight.shape, bf16),
        pltpu.VMEM(gate_w.shape[1:], bf16),
        pltpu.VMEM(up_w.shape[1:], bf16),
        pltpu.VMEM(down_w.shape[1:], bf16),
        pltpu.VMEM((2, tokens, width), bf16),
        pltpu.VMEM((chips, 2, subs, few, width), bf16),
        pltpu.VMEM((chips, 2, subs, 2, few, width), bf16),
        pltpu.VMEM((2 * cap, units), bf16),
        pltpu.VMEM((chips, 2, 2, cap, width), bf16),
        pltpu.VMEM((chips, 2, cap, width), bf16),
        pltpu.VMEM((chips, cap, width), bf16),
        pltpu.VMEM((chips, cap, width), bf16),
        pltpu.VMEM((chips, cap, width), bf16),
        pltpu.VMEM((chips, cap, width), bf16),
        pltpu.VMEM((chips // 2, 2, cap, width), bf16),
        pltpu.VMEM((chips // 2, 2, cap, width), bf16),
        pltpu.VMEM((tokens, width), bf16),
        pltpu.VMEM((tokens, width), bf16),
        pltpu.VMEM((chips, 2, tokens, cap), bf16),
        pltpu.VMEM((tokens, width), f32),
        pltpu.VMEM((local // LANES, halo + length, LANES), f32),
        pltpu.VMEM((halo, local), bf16),
        pltpu.VMEM((halo, local), bf16),
        pltpu.VMEM((2, length, local), bf16),
        dma((4,)),
        dma((8,)),
        dma((chips, 2, subs)),
        dma((chips, 2, subs)),
        dma((chips, subs)),
        dma((chips, subs)),
        dma((chips, 2, subs)),
        dma((chips, 2, subs)),
        dma((chips, 2, subs)),
        dma((chips, 2, subs)),
        dma((chips, subs)),
        dma((chips, subs)),
        dma((chips, subs)),
        dma((chips, subs)),
        dma((chips // 2, 2)),
        dma((chips // 2, 2)),
        dma((1,)),
        dma((1,)),
        dma((pieces,)),
        dma((pieces,)),
        dma((1,)),
        dma((1,)),
    ]
    return pl.pallas_call(
        functools.partial(step_kernel, chips, cap, subs, pieces, halo),
        out_shape=(
            jax.ShapeDtypeStruct((length, out_weight.shape[1]), bf16),
            jax.ShapeDtypeStruct((tokens, width), bf16),
        ),
        in_specs=[hbm] * 12,
        out_specs=(vmem, vmem),
        scratch_shapes=scratch,
        compiler_params=pltpu.CompilerParams(
            collective_id=0, has_side_effects=True, vmem_limit_bytes=40 * 1024 * 1024
        ),
    )(
        *(
            pltpu.with_memory_space_constraint(value, pltpu.HBM)
            for value in (
                value_in,
                gate_in,
                conv_taps,
                chan_gain.reshape(1, -1),
                out_weight,
                second_rows,
                expert_gain.reshape(1, -1),
                routes.T,
                route_weights.T,
                gate_w,
                up_w,
                down_w,
            )
        )
    )


def solution(mesh):
    chips = mesh.shape["ep"] // 2
    paired = mesh.shape["tp"] == 2 and chips > 1 and chips & (chips - 1) == 0
    placed = (
        P(("grp", "ep"), "tp"),
        P(("grp", "ep"), "tp"),
        P(None, "tp"),
        P(),
        P(None, "tp"),
        P(("grp", "ep"), None),
        P(),
        P(("grp", "ep"), None),
        P(("grp", "ep"), None),
        P("ep", None, "tp"),
        P("ep", None, "tp"),
        P("ep", "tp", None),
    )
    return jax.shard_map(
        one_kernel if paired else on_device,
        mesh=mesh,
        in_specs=placed,
        out_specs=(P(("grp", "ep"), "tp"), P(("grp", "ep"), "tp")),
        check_vma=False,
    )
```

```python
import functools

import jax
import jax.numpy as jnp
from jax import lax
from jax.experimental import pallas as pl
from jax.experimental.pallas import tpu as pltpu
from jax.sharding import PartitionSpec as P

eps = 1e-06
LANES = 128
MESH = pl.DeviceIdType.MESH


def partner_2(value, axis, bit):
    return lax.ppermute(value, axis, [(i, i ^ 1 << bit) for i in range(lax.axis_size(axis))])


def shifted(value, axis, by):
    devices = lax.axis_size(axis)
    pairs = [(i, i + by) for i in range(devices) if 0 <= i + by < devices]
    return lax.ppermute(value, axis, pairs)


def partner(block):
    return partner_2(block, "ep", 0)


def across(block):
    return lax.all_to_all(block, "ep", split_axis=0, concat_axis=0, tiled=True)


def on_device(
    value_in,
    gate_in,
    conv_taps,
    chan_gain,
    out_weight,
    second_rows,
    expert_gain,
    routes,
    route_weights,
    gate_w,
    up_w,
    down_w,
):
    taps = conv_taps.shape[0]
    glu = (value_in.astype(jnp.float32) * jax.nn.sigmoid(gate_in.astype(jnp.float32))).astype(
        jnp.bfloat16
    )
    length = glu.shape[0]
    before = shifted(glu[length - taps + 1 :], "ep", 1)
    padded = jnp.concatenate([before, glu], axis=0).astype(jnp.float32)
    total = jnp.zeros(glu.shape, jnp.float32)
    for offset in range(taps):
        total = total + conv_taps[offset][None, :] * padded[offset : offset + length]
    convolved = total.astype(jnp.bfloat16)
    channels = lax.all_gather(convolved, "tp", axis=1, tiled=True)
    values = channels.astype(jnp.float32)
    centered = values - jnp.mean(values, axis=-1, keepdims=True)
    scaled = (
        centered
        * lax.rsqrt(jnp.mean(centered * centered, axis=-1, keepdims=True) + eps)
        * chan_gain
    )
    activated = jax.nn.silu(scaled).astype(jnp.bfloat16)
    mixer_rows = jnp.dot(activated, out_weight, preferred_element_type=jnp.float32).astype(
        jnp.bfloat16
    )
    n_ep = lax.axis_size("ep")
    experts = n_ep // 2
    tokens = second_rows.shape[0]
    top = routes.shape[1]
    width = second_rows.shape[1]
    capacity = 2 * max(1, min(tokens // 2, 3 * tokens * top // (4 * experts)))
    half_slots = capacity // 2
    rows = second_rows.astype(jnp.float32)
    normed = (
        rows * lax.rsqrt(jnp.mean(rows * rows, axis=-1, keepdims=True) + eps) * expert_gain
    ).astype(jnp.bfloat16)
    chosen = routes.reshape(-1)
    hits = (chosen[:, None] == jnp.arange(experts, dtype=jnp.int32)[None, :]).astype(jnp.int32)
    place = jnp.sum((jnp.cumsum(hits, axis=0) - 1) * hits, axis=1)
    target = (chosen * capacity + place).reshape(tokens, top)
    slots = jnp.arange(experts * capacity, dtype=jnp.int32)
    matches = target[:, :, None] == slots[None, None, :]
    picker = jnp.any(matches, axis=1).astype(jnp.bfloat16)
    outgoing = jnp.dot(picker.T, normed, preferred_element_type=jnp.float32).astype(jnp.bfloat16)
    combiner = jnp.sum(jnp.where(matches, route_weights[:, :, None], 0.0), axis=1)
    upper = lax.axis_index("ep") % 2
    arrived = across(outgoing.reshape(n_ep, half_slots, width))
    other = partner(arrived)
    first = jnp.where(upper == 0, arrived, other)
    second = jnp.where(upper == 0, other, arrived)
    incoming = jnp.concatenate([first, second], axis=1)
    block_rows = incoming.reshape(n_ep * capacity, width)
    gate = jnp.dot(block_rows, gate_w[0], preferred_element_type=jnp.float32)
    lifted = jnp.dot(block_rows, up_w[0], preferred_element_type=jnp.float32)
    hidden = (jax.nn.silu(gate) * lifted).astype(jnp.bfloat16)
    partial_value = jnp.dot(hidden, down_w[0], preferred_element_type=jnp.float32)
    half_sums = lax.psum_scatter(
        partial_value.astype(jnp.bfloat16), "tp", scatter_dimension=1, tiled=True
    )
    columns = half_sums.shape[1]
    half_sums = half_sums.reshape(n_ep, capacity, columns)
    other_sums = partner(half_sums)
    joined = (half_sums.astype(jnp.float32) + other_sums.astype(jnp.float32)).astype(jnp.bfloat16)
    own = lax.dynamic_slice_in_dim(joined, upper * half_slots, half_slots, 1)
    results = across(own).reshape(experts * capacity, columns)
    routed_rows = jnp.dot(
        combiner,
        results.astype(jnp.float32),
        precision=lax.Precision.HIGHEST,
        preferred_element_type=jnp.float32,
    ).astype(jnp.bfloat16)
    return (mixer_rows, routed_rows)


def _xor(value, mask):
    out, bit = value, 1
    while bit <= mask:
        if mask & bit:
            out = out + bit - 2 * bit * lax.rem(lax.div(value, bit), 2)
        bit *= 2
    return out


def _iota(shape, dim):
    return lax.broadcasted_iota(jnp.int32, shape, dim)


def _dot(a, b):
    return jnp.dot(a, b, preferred_element_type=jnp.float32)


def step_kernel(
    chips,
    cap,
    subs,
    pieces,
    halo,
    value_hbm,
    gate_hbm,
    taps_hbm,
    gain_hbm,
    wo_hbm,
    rows_hbm,
    egain_hbm,
    routes_hbm,
    rw_hbm,
    wg_hbm,
    wu_hbm,
    wd_hbm,
    mixer_ref,
    routed_ref,
    value_ref,
    gate_ref,
    taps_ref,
    gain_ref,
    rows_ref,
    egain_ref,
    routes_t_ref,
    rw_t_ref,
    wo,
    wg,
    wu,
    wd,
    normed,
    picked,
    block,
    hid,
    part,
    pair_in,
    cross_out,
    cross_in,
    back_out,
    results,
    near_out,
    near_res,
    q_out,
    q_in,
    combs,
    acc,
    glu,
    halo_out,
    halo_in,
    conv,
    w_sem,
    in_sem,
    far_recv,
    near_recv,
    xf_recv,
    cf_recv,
    cw_recv,
    r1_recv,
    r2_recv,
    r3_recv,
    r4_recv,
    q_recv,
    ag_recv,
    halo_recv,
    sent,
):
    f32, bf16 = jnp.float32, jnp.bfloat16
    ep = lax.axis_index("ep")
    x = lax.axis_index("tp")
    n_ep = 2 * chips
    z, c = lax.div(ep, 2), lax.rem(ep, 2)
    width = block.shape[-1]
    tokens = rows_ref.shape[0]
    length, local = value_ref.shape
    cols = local // LANES
    ntaps = taps_ref.shape[0]
    few = cap // subs
    split_from = max(1, chips // 2)
    far = list(range(split_from, chips))
    near = list(range(1, split_from))
    swap = 1 - lax.rem(z + lax.div(z, 2), 2)
    peers = [_xor(z, k) for k in range(chips)]
    for k in far:
        peers[k] = peers[k] + swap * (1 - 2 * lax.rem(peers[k], 2))

    def dev(zd, cd, xd):
        return {"ep": zd * 2 + cd, "tp": xd}

    def remote(src, dst, send, recv, to):
        return pltpu.make_async_remote_copy(
            src_ref=src, dst_ref=dst, send_sem=send, recv_sem=recv, device_id=to, device_id_type=MESH
        )

    to_send = {
        name: sent.at[i]
        for i, name in enumerate(["disp", "core", "pair", "cross", "back", "ag", "q", "halo"])
    }
    wing = lax.rem(z, chips // 2)
    core_peer = dev(z, 1 - c, x)
    plane_peer = dev(z, c, 1 - x)
    after = {"ep": lax.rem(ep + 1, n_ep), "tp": x}
    prior = {"ep": lax.rem(ep + n_ep - 1, n_ep), "tp": x}
    barrier = pltpu.get_barrier_semaphore()
    greeted = [core_peer, plane_peer, after, prior] + [dev(peers[k], c, x) for k in range(1, chips)]
    for to in greeted:
        pl.semaphore_signal(barrier, inc=1, device_id=to, device_id_type=MESH)

    inputs = [
        (rows_hbm, rows_ref),
        (routes_hbm, routes_t_ref),
        (rw_hbm, rw_t_ref),
        (egain_hbm, egain_ref),
        (value_hbm, value_ref),
        (gate_hbm, gate_ref),
        (taps_hbm, taps_ref),
        (gain_hbm, gain_ref),
    ]
    inputs = [pltpu.make_async_copy(a, b, in_sem.at[i]) for i, (a, b) in enumerate(inputs)]
    weights = [
        pltpu.make_async_copy(wg_hbm.at[0], wg, w_sem.at[0]),
        pltpu.make_async_copy(wu_hbm.at[0], wu, w_sem.at[1]),
        pltpu.make_async_copy(wd_hbm.at[0], wd, w_sem.at[2]),
        pltpu.make_async_copy(wo_hbm, wo, w_sem.at[3]),
    ]
    for copy in inputs:
        copy.start()
    for copy in inputs[:4]:
        copy.wait()
    erows = -(-chips // 8) * 8
    r0t, r1t = routes_t_ref[0:1, :], routes_t_ref[1:2, :]
    eid = _iota((erows, tokens), 0)
    hits_t = (r0t == eid) | (r1t == eid)
    earlier_t = (_iota((tokens, tokens), 0) < _iota((tokens, tokens), 1)).astype(f32)
    place_t = _dot(hits_t.astype(f32).astype(bf16), earlier_t.astype(bf16))
    slot_t = jnp.where(hits_t, place_t, -1.0).astype(jnp.int32)

    rows = rows_ref[...].astype(f32)
    scale = lax.rsqrt(jnp.mean(rows * rows, axis=-1, keepdims=True) + eps)
    both = (rows * scale * egain_ref[...]).astype(bf16)
    normed[0] = both[:, :width]
    normed[1] = both[:, width:]

    slots = _iota((cap, tokens), 0)

    def pick(k):
        row = jnp.sum(jnp.where(eid == peers[k], slot_t, 0), axis=0, keepdims=True)
        return (slots == row).astype(f32).astype(bf16)

    def cut(s):
        return slice(s * few, (s + 1) * few)

    for k in far:
        rows_k = _dot(pick(k), normed[x]).astype(bf16)
        for s in range(subs):
            picked[k, 0, s] = rows_k[cut(s)]
    for copy in inputs[4:]:
        copy.wait()
    for copy in weights:
        copy.start()
    last = slice(length - halo, length)
    gated = value_ref[last, :].astype(f32) * jax.nn.sigmoid(gate_ref[last, :].astype(f32))
    halo_out[...] = gated.astype(bf16)

    pl.semaphore_wait(barrier, len(greeted))
    halo_copy = remote(halo_out, halo_in, to_send["halo"], halo_recv.at[0], after)
    halo_copy.start()

    def far_copy(k, s, at):
        return remote(
            picked.at[k, 0, s],
            block.at[at, x, s, c],
            to_send["disp"],
            far_recv.at[lax.rem(at, chips // 2), s],
            dev(peers[k], c, x),
        )

    def near_dispatch(k, at):
        return remote(
            picked.at[k],
            block.at[at, :, :, c],
            to_send["disp"],
            near_recv.at[k - 1],
            dev(peers[k], c, x),
        )

    def core_copy(k, h, s, core):
        here = block.at[peers[k], h, s, core]
        return remote(here, here, to_send["core"], cf_recv.at[k - split_from, h, s], core_peer)

    def core_copies(k, core):
        here = block.at[peers[k], :, :, core]
        return remote(here, here, to_send["core"], cw_recv.at[k], core_peer)

    def plane_copy(k, h, s):
        here = block.at[peers[k], h, s, c]
        return remote(here, here, to_send["cross"], xf_recv.at[k - split_from, s], plane_peer)

    def from_core(k, h, s):
        core_copy(k, h, s, 1 - c).wait_recv()

    def slot_of_pair(k, s):
        return k if k < split_from else split_from + (k - split_from) * subs + s

    def pair_copy(k, o, s, n):
        h = x if o else 1 - x
        span = pl.ds(s * few, n)
        return remote(
            part.at[k, 1 - c, h, span],
            pair_in.at[k, h, span],
            to_send["pair"],
            r1_recv.at[slot_of_pair(k, s), o],
            core_peer,
        )

    def cross_copy(k, s, n):
        span = pl.ds(s * few, n)
        return remote(
            cross_out.at[k, span],
            cross_in.at[k, span],
            to_send["cross"],
            r2_recv.at[k - split_from, s],
            plane_peer,
        )

    def back_copy(k, s, n, at):
        span = pl.ds(s * few, n)
        return remote(
            back_out.at[k, span],
            results.at[at, span],
            to_send["back"],
            r3_recv.at[lax.rem(at, chips // 2), s],
            dev(peers[k], c, x),
        )

    def feed_forward(k, s, n, between=None, after_half=None):
        count = n // few
        zs = peers[k]
        a0 = block[zs, 0, s : s + count].reshape(2 * n, width)
        a1 = block[zs, 1, s : s + count].reshape(2 * n, width)
        units = hid.shape[1]
        step = min(units, 256)
        for j in range(0, units, step):
            gate = _dot(a0, wg[:width, j : j + step]) + _dot(a1, wg[width:, j : j + step])
            up = _dot(a0, wu[:width, j : j + step]) + _dot(a1, wu[width:, j : j + step])
            hid[: 2 * n, j : j + step] = (gate * jax.nn.sigmoid(gate) * up).astype(bf16)
        if between:
            between()
        h_all = hid[: 2 * n, :]
        for o in range(2):
            if o and after_half:
                after_half()
            h = x if o else 1 - x
            for j in range(0, width, step):
                at = pl.ds(pl.multiple_of(h * width + j, step), step)
                out = _dot(h_all, wd[:, at]).astype(bf16)
                for i in range(count):
                    for core in range(2):
                        r = (2 * i + core) * few
                        part[k, core, h, cut(s + i), j : j + step] = out[r : r + few]
            pair_copy(k, o, s, n).start()

    def pair_sum(k, s, n, wait=True):
        if wait:
            pair_copy(k, 0, s, n).wait_recv()
        span = slice(s * few, s * few + n)
        total = part[k, c, 1 - x, span].astype(f32) + pair_in[k, 1 - x, span].astype(f32)
        cross_out[k, span] = total.astype(bf16)
        cross_copy(k, s, n).start()

    def plane_sum(k, s, n, wait=True):
        if wait:
            pair_copy(k, 1, s, n).wait_recv()
        cross_copy(k, s, n).wait_recv()
        span = slice(s * few, s * few + n)
        total = (
            part[k, c, x, span].astype(f32)
            + pair_in[k, x, span].astype(f32)
            + cross_in[k, span].astype(f32)
        )
        back_out[k, span] = total.astype(bf16)
        back_copy(k, s, n, z).start()

    def near_copy(k, o):
        return remote(
            near_out.at[k, o],
            near_res.at[k, o],
            to_send["back"],
            r4_recv.at[k - 1, o],
            dev(peers[k], c, x),
        )

    def near_sum(k, o):
        pair_copy(k, o, 0, cap).wait_recv()
        h = x if o else 1 - x
        total = part[k, c, h].astype(f32) + pair_in[k, h].astype(f32)
        near_out[k, o] = total.astype(bf16)
        if k:
            near_copy(k, o).start()

    q_copy = remote(q_out, q_in, to_send["q"], q_recv.at[0], plane_peer)

    def close(o):
        total = weighed(0, near_out[0, o])
        for k in near:
            near_copy(k, o).wait_recv()
            total = total + weighed(k, near_res[k, o])
        if o:
            acc[...] = total
        else:
            q_out[...] = total.astype(bf16)
            q_copy.start()

    def pair_sums(k):
        pair_copy(k, 0, 0, cap).wait_recv()
        for s in range(subs):
            pair_sum(k, s, few, False)

    def plane_sums(k):
        pair_copy(k, 1, 0, cap).wait_recv()
        for s in range(subs):
            plane_sum(k, s, few, False)

    def send_far():
        for s in range(subs):
            for k in far:
                far_copy(k, s, z).start()

    def far_in(k, s):
        far_copy(k, s, peers[k]).wait_recv()
        plane_copy(k, x, s).start()
        core_copy(k, x, s, c).start()

    def far_over(k, s):
        plane_copy(k, 1 - x, s).wait_recv()
        core_copy(k, 1 - x, s, c).start()

    def near_in(k):
        near_dispatch(k, peers[k]).wait_recv()
        core_copies(k, c).start()

    def from_cores(k):
        if k < split_from:
            core_copies(k, 1 - c).wait_recv()
        else:
            for h in range(2):
                for s in range(subs):
                    from_core(k, h, s)

    def weighed(k, found):
        return _dot(combs[k, 0], found) + _dot(combs[k, 1], found)

    rows_per = length // pieces
    tile = 64 if rows_per % 64 == 0 else rows_per

    early = min(pieces, 4)
    groups = [(p, p + 1) for p in range(1, early)]
    groups += [(p, min(p + 2, pieces)) for p in range(early, pieces, 2)] + [(0, 1)]
    gathered = set()

    def gather_copy(g, who):
        lo, hi = groups[g]
        rows_g = conv.at[who, pl.ds(lo * rows_per, (hi - lo) * rows_per)]
        return remote(rows_g, rows_g, to_send["ag"], ag_recv.at[g], plane_peer)

    def gather(lo, hi):
        for g in range(lo, hi):
            gather_copy(g, x).start()

    def convolve(lo, hi, send=False):
        def conv_tile(r, carry):
            r0 = pl.multiple_of(r * tile, tile)
            for i in range(cols):
                total = jnp.zeros((tile, LANES), f32)
                for k in range(ntaps):
                    total = (
                        total
                        + taps_ref[k : k + 1, i * LANES : (i + 1) * LANES]
                        * glu[i, pl.ds(r0 + (k + halo - ntaps + 1), tile), :]
                    )
                conv[x, pl.ds(r0, tile), i * LANES : (i + 1) * LANES] = total.astype(bf16)
            if send:
                rows_r = conv.at[x, pl.ds(r0, tile)]
                remote(rows_r, rows_r, to_send["ag"], ag_recv.at[r - 1], plane_peer).start()
            return carry

        per = rows_per // tile
        send = send and per == 1
        lax.fori_loop(lo * per, hi * per, conv_tile, 0)
        return send

    def mix(lo, hi):
        for g, (first, last) in enumerate(groups):
            if g not in gathered and first < hi and last > lo:
                gather_copy(g, 1 - x).wait_recv()
                gathered.add(g)
        here = slice(lo * rows_per, hi * rows_per)
        first, second = conv[0, here, :].astype(f32), conv[1, here, :].astype(f32)
        count = 2 * local
        mean = (
            jnp.sum(first, axis=-1, keepdims=True) + jnp.sum(second, axis=-1, keepdims=True)
        ) / count
        first, second = first - mean, second - mean
        var = (
            jnp.sum(first * first, axis=-1, keepdims=True)
            + jnp.sum(second * second, axis=-1, keepdims=True)
        ) / count
        scale = lax.rsqrt(var + eps)
        first = first * scale * gain_ref[:, :local]
        second = second * scale * gain_ref[:, local:]
        first = (first * jax.nn.sigmoid(first)).astype(bf16)
        second = (second * jax.nn.sigmoid(second)).astype(bf16)
        mixer_ref[here, :] = (_dot(first, wo[:local, :]) + _dot(second, wo[local:, :])).astype(bf16)

    def combine(k):
        return acc[...] + weighed(k, results[peers[k]])

    def returned(k, n):
        for s in range(subs):
            back_copy(k, s, n, peers[k]).wait_recv()

    send_far()
    for k in near:
        rows_k = [_dot(pick(k), normed[h]).astype(bf16) for h in range(2)]
        for h in range(2):
            for s in range(subs):
                picked[k, h, s] = rows_k[h][cut(s)]
        near_dispatch(k, z).start()
    for h in range(2):
        rows_0 = _dot(pick(0), normed[h]).astype(bf16)
        for s in range(subs):
            block[z, h, s, c] = rows_0[cut(s)]
    core_copies(0, c).start()
    kept = slice(0, length - halo)
    for i in range(cols):
        at = slice(i * LANES, (i + 1) * LANES)
        gated = value_ref[kept, at].astype(f32) * jax.nn.sigmoid(gate_ref[kept, at].astype(f32))
        glu[i, halo:length, :] = gated.astype(bf16).astype(f32)
        glu[i, length:, :] = halo_out[:, at].astype(f32)
    if not convolve(1, early, True):
        gather(0, early - 1)
    convolve(early, pieces)
    mid_far, last_far = far[:-1], far[-1]
    units = [(k, s) for k in mid_far for s in range(subs)]
    lane = _iota((tokens, LANES), 1)
    index = _iota((8, tokens), 0)
    rows_named = jnp.where(index == 0, r0t, 0).astype(f32) + jnp.where(index == 1, r1t, 0).astype(f32)
    for j in range(2):
        rows_named = rows_named + jnp.where(index == 2 + j, rw_t_ref[j : j + 1, :], 0.0)
    named = jnp.transpose(rows_named)
    r0, r1 = (named[:, j : j + 1].astype(jnp.int32) for j in range(2))
    hits = ((r0 == lane) | (r1 == lane)).astype(f32).astype(bf16)
    earlier = (_iota((tokens, tokens), 1) < _iota((tokens, tokens), 0)).astype(f32).astype(bf16)
    place = _dot(earlier, hits)
    slot_of = _iota((tokens, cap), 1)
    places = [
        jnp.sum(jnp.where(lane == r, place, 0.0), axis=1, keepdims=True).astype(jnp.int32)
        for r in (r0, r1)
    ]
    for k in range(chips):
        comb = jnp.zeros((tokens, cap), f32)
        for j, r in enumerate((r0, r1)):
            mine = jnp.where(r == peers[k], places[j], -1)
            comb = comb + jnp.where(slot_of == mine, named[:, 2 + j : 3 + j], 0.0)
        head = comb.astype(bf16)
        combs[k, 0] = head
        combs[k, 1] = (comb - head.astype(f32)).astype(bf16)


    halo_copy.wait_recv()
    before = jnp.where(ep > 0, halo_in[...].astype(f32), 0.0)
    for i in range(cols):
        glu[i, :halo, :] = before[:, i * LANES : (i + 1) * LANES]
    convolve(0, 1)
    for copy in weights[:3]:
        copy.wait()
    from_cores(0)
    feed_forward(0, 0, cap, lambda: far_in(*units[0]))
    far_over(*units[0])
    for unit in units[1:]:
        far_in(*unit)
    later = min(len(groups), early)
    gather(early - 1, later)
    for o in range(2):
        near_sum(0, o)
    for h in range(2):
        from_core(units[0][0], h, units[0][1])
    feed_forward(*units[0], few, lambda: far_in(last_far, 0))

    def near_ins():
        for k in near:
            near_in(k)

    def last_ins():
        for s in range(1, subs):
            far_in(last_far, s)

    if len(units) == 1:
        near_ins()
        last_ins()
    for i in range(1, len(units)):
        far_over(*units[i])
        pair_sum(*units[i - 1], few)
        for h in range(2):
            from_core(units[i][0], h, units[i][1])
        only = i == 1
        feed_forward(*units[i], few, near_ins if only else None, last_ins if only else None)
    far_over(last_far, 0)
    for k in near:
        from_cores(k)

    def first_back():
        pair_sum(*units[-1], few)
        plane_sum(*units[0], few)

    for k in near:
        feed_forward(k, 0, cap, first_back if k == near[0] else None)
    gather(later, len(groups))
    for s in range(1, subs):
        far_over(last_far, s)
    for k in near:
        near_sum(k, 0)
    from_cores(last_far)

    def near_rest():
        for k in near:
            near_sum(k, 1)

    def second_back():
        for unit in units[1:]:
            plane_sum(*unit, few)

    feed_forward(last_far, 0, cap, near_rest, second_back)
    pair_sums(last_far)
    weights[3].wait()
    group = 2 if pieces % 2 == 0 else 1
    for p in range(group, pieces, group):
        mix(p, p + group)

    def close_first():
        close(0)

    pl.when(swap == 0)(close_first)
    plane_sums(last_far)
    pl.when(swap == 1)(close_first)
    mix(0, group)
    close(1)
    for k in far[:-1]:
        returned(k, few)
        acc[...] = combine(k)
    q_copy.wait_recv()
    acc[...] = acc[...] + q_in[...].astype(f32)
    returned(far[-1], few)
    routed_ref[...] = combine(far[-1]).astype(bf16)

    half = block.at[pl.ds(0, chips // 2)]
    for name, ref in (
        ("disp", block.at[0]),
        ("core", half),
        ("pair", half),
        ("cross", block.at[0]),
        ("back", block.at[0]),
        ("ag", conv.at[0]),
        ("q", q_out),
        ("halo", halo_out),
    ):
        remote(ref, ref, to_send[name], halo_recv.at[0], core_peer).wait_send()


def store_kernel(mixer_ref, routed_ref, mixer_hbm, routed_hbm, sem):
    copies = [
        pltpu.make_async_copy(mixer_ref, mixer_hbm, sem.at[0]),
        pltpu.make_async_copy(routed_ref, routed_hbm, sem.at[1]),
    ]
    for copy in copies:
        copy.start()
    for copy in copies:
        copy.wait()


def one_kernel(
    value_in,
    gate_in,
    conv_taps,
    chan_gain,
    out_weight,
    second_rows,
    expert_gain,
    routes,
    route_weights,
    gate_w,
    up_w,
    down_w,
):
    chips = lax.axis_size("ep") // 2
    tokens, model = second_rows.shape
    top = routes.shape[1]
    width = model // 2
    cap = 2 * max(1, min(tokens // 2, 3 * tokens * top // (4 * chips)))
    subs = 2 if cap % 32 == 0 else 1
    few = cap // subs
    length, local = value_in.shape
    units = gate_w.shape[2]
    halo = -(-(conv_taps.shape[0] - 1) // 16) * 16
    pieces = 8 if length % 128 == 0 and length // 8 > halo else 1
    bf16, f32 = jnp.bfloat16, jnp.float32
    vmem = pl.BlockSpec(memory_space=pltpu.VMEM)
    hbm = pl.BlockSpec(memory_space=pltpu.HBM)
    dma = pltpu.SemaphoreType.DMA
    scratch = [
        pltpu.VMEM(value_in.shape, bf16),
        pltpu.VMEM(gate_in.shape, bf16),
        pltpu.VMEM(conv_taps.shape, f32),
        pltpu.VMEM((1, chan_gain.shape[0]), f32),
        pltpu.VMEM(second_rows.shape, bf16),
        pltpu.VMEM((1, model), f32),
        pltpu.VMEM((top, tokens), jnp.int32),
        pltpu.VMEM((top, tokens), f32),
        pltpu.VMEM(out_weight.shape, bf16),
        pltpu.VMEM(gate_w.shape[1:], bf16),
        pltpu.VMEM(up_w.shape[1:], bf16),
        pltpu.VMEM(down_w.shape[1:], bf16),
        pltpu.VMEM((2, tokens, width), bf16),
        pltpu.VMEM((chips, 2, subs, few, width), bf16),
        pltpu.VMEM((chips, 2, subs, 2, few, width), bf16),
        pltpu.VMEM((2 * cap, units), bf16),
        pltpu.VMEM((chips, 2, 2, cap, width), bf16),
        pltpu.VMEM((chips, 2, cap, width), bf16),
        pltpu.VMEM((chips, cap, width), bf16),
        pltpu.VMEM((chips, cap, width), bf16),
        pltpu.VMEM((chips, cap, width), bf16),
        pltpu.VMEM((chips, cap, width), bf16),
        pltpu.VMEM((chips // 2, 2, cap, width), bf16),
        pltpu.VMEM((chips // 2, 2, cap, width), bf16),
        pltpu.VMEM((tokens, width), bf16),
        pltpu.VMEM((tokens, width), bf16),
        pltpu.VMEM((chips, 2, tokens, cap), bf16),
        pltpu.VMEM((tokens, width), f32),
        pltpu.VMEM((local // LANES, halo + length, LANES), f32),
        pltpu.VMEM((halo, local), bf16),
        pltpu.VMEM((halo, local), bf16),
        pltpu.VMEM((2, length, local), bf16),
        dma((4,)),
        dma((8,)),
        dma((chips // 2, subs)),
        dma((chips // 2 - 1,)),
        dma((chips // 2, subs)),
        dma((chips // 2, 2, subs)),
        dma((chips // 2,)),
        dma((chips // 2 + (chips // 2 - 1) * subs + 1, 2)),
        dma((chips // 2, subs)),
        dma((chips // 2, subs)),
        dma((chips // 2 - 1, 2)),
        dma((1,)),
        dma((min(pieces, 4) + (pieces - min(pieces, 4) + 1) // 2,)),
        dma((1,)),
        dma((8,)),
    ]
    outs = pl.pallas_call(
        functools.partial(step_kernel, chips, cap, subs, pieces, halo),
        out_shape=(
            jax.ShapeDtypeStruct((length, out_weight.shape[1]), bf16),
            jax.ShapeDtypeStruct((tokens, width), bf16),
        ),
        in_specs=[hbm] * 12,
        out_specs=(vmem, vmem),
        scratch_shapes=scratch,
        compiler_params=pltpu.CompilerParams(
            collective_id=0, has_side_effects=True, vmem_limit_bytes=40 * 1024 * 1024
        ),
    )(
        *(
            pltpu.with_memory_space_constraint(value, pltpu.HBM)
            for value in (
                value_in,
                gate_in,
                conv_taps,
                chan_gain.reshape(1, -1),
                out_weight,
                second_rows,
                expert_gain.reshape(1, -1),
                routes.T,
                route_weights.T,
                gate_w,
                up_w,
                down_w,
            )
        )
    )
    return pl.pallas_call(
        store_kernel,
        out_shape=tuple(jax.ShapeDtypeStruct(out.shape, out.dtype) for out in outs),
        in_specs=[vmem] * 2,
        out_specs=(pl.BlockSpec(memory_space=pl.ANY),) * 2,
        scratch_shapes=[dma((2,))],
        compiler_params=pltpu.CompilerParams(vmem_limit_bytes=1024 * 1024),
    )(*outs)


def solution(mesh):
    chips = mesh.shape["ep"] // 2
    paired = mesh.shape["tp"] == 2 and chips == 4
    placed = (
        P(("grp", "ep"), "tp"),
        P(("grp", "ep"), "tp"),
        P(None, "tp"),
        P(),
        P(None, "tp"),
        P(("grp", "ep"), None),
        P(),
        P(("grp", "ep"), None),
        P(("grp", "ep"), None),
        P("ep", None, "tp"),
        P("ep", None, "tp"),
        P("ep", "tp", None),
    )
    return jax.shard_map(
        one_kernel if paired else on_device,
        mesh=mesh,
        in_specs=placed,
        out_specs=(P(("grp", "ep"), "tp"), P(("grp", "ep"), "tp")),
        check_vma=False,
    )
```

```python
import functools

import jax
import jax.numpy as jnp
from jax import lax
from jax.experimental import pallas as pl
from jax.experimental.pallas import tpu as pltpu
from jax.sharding import PartitionSpec as P

eps = 1e-06
LANES = 128
MESH = pl.DeviceIdType.MESH


def partner_2(value, axis, bit):
    return lax.ppermute(value, axis, [(i, i ^ 1 << bit) for i in range(lax.axis_size(axis))])


def shifted(value, axis, by):
    devices = lax.axis_size(axis)
    pairs = [(i, i + by) for i in range(devices) if 0 <= i + by < devices]
    return lax.ppermute(value, axis, pairs)


def partner(block):
    return partner_2(block, "ep", 0)


def across(block):
    return lax.all_to_all(block, "ep", split_axis=0, concat_axis=0, tiled=True)


def on_device(
    value_in,
    gate_in,
    conv_taps,
    chan_gain,
    out_weight,
    second_rows,
    expert_gain,
    routes,
    route_weights,
    gate_w,
    up_w,
    down_w,
):
    taps = conv_taps.shape[0]
    glu = (value_in.astype(jnp.float32) * jax.nn.sigmoid(gate_in.astype(jnp.float32))).astype(
        jnp.bfloat16
    )
    length = glu.shape[0]
    before = shifted(glu[length - taps + 1 :], "ep", 1)
    padded = jnp.concatenate([before, glu], axis=0).astype(jnp.float32)
    total = jnp.zeros(glu.shape, jnp.float32)
    for offset in range(taps):
        total = total + conv_taps[offset][None, :] * padded[offset : offset + length]
    convolved = total.astype(jnp.bfloat16)
    channels = lax.all_gather(convolved, "tp", axis=1, tiled=True)
    values = channels.astype(jnp.float32)
    centered = values - jnp.mean(values, axis=-1, keepdims=True)
    scaled = (
        centered
        * lax.rsqrt(jnp.mean(centered * centered, axis=-1, keepdims=True) + eps)
        * chan_gain
    )
    activated = jax.nn.silu(scaled).astype(jnp.bfloat16)
    mixer_rows = jnp.dot(activated, out_weight, preferred_element_type=jnp.float32).astype(
        jnp.bfloat16
    )
    n_ep = lax.axis_size("ep")
    experts = n_ep // 2
    tokens = second_rows.shape[0]
    top = routes.shape[1]
    width = second_rows.shape[1]
    capacity = 2 * max(1, min(tokens // 2, 3 * tokens * top // (4 * experts)))
    half_slots = capacity // 2
    rows = second_rows.astype(jnp.float32)
    normed = (
        rows * lax.rsqrt(jnp.mean(rows * rows, axis=-1, keepdims=True) + eps) * expert_gain
    ).astype(jnp.bfloat16)
    chosen = routes.reshape(-1)
    hits = (chosen[:, None] == jnp.arange(experts, dtype=jnp.int32)[None, :]).astype(jnp.int32)
    place = jnp.sum((jnp.cumsum(hits, axis=0) - 1) * hits, axis=1)
    target = (chosen * capacity + place).reshape(tokens, top)
    slots = jnp.arange(experts * capacity, dtype=jnp.int32)
    matches = target[:, :, None] == slots[None, None, :]
    picker = jnp.any(matches, axis=1).astype(jnp.bfloat16)
    outgoing = jnp.dot(picker.T, normed, preferred_element_type=jnp.float32).astype(jnp.bfloat16)
    combiner = jnp.sum(jnp.where(matches, route_weights[:, :, None], 0.0), axis=1)
    upper = lax.axis_index("ep") % 2
    arrived = across(outgoing.reshape(n_ep, half_slots, width))
    other = partner(arrived)
    first = jnp.where(upper == 0, arrived, other)
    second = jnp.where(upper == 0, other, arrived)
    incoming = jnp.concatenate([first, second], axis=1)
    block_rows = incoming.reshape(n_ep * capacity, width)
    gate = jnp.dot(block_rows, gate_w[0], preferred_element_type=jnp.float32)
    lifted = jnp.dot(block_rows, up_w[0], preferred_element_type=jnp.float32)
    hidden = (jax.nn.silu(gate) * lifted).astype(jnp.bfloat16)
    partial_value = jnp.dot(hidden, down_w[0], preferred_element_type=jnp.float32)
    half_sums = lax.psum_scatter(
        partial_value.astype(jnp.bfloat16), "tp", scatter_dimension=1, tiled=True
    )
    columns = half_sums.shape[1]
    half_sums = half_sums.reshape(n_ep, capacity, columns)
    other_sums = partner(half_sums)
    joined = (half_sums.astype(jnp.float32) + other_sums.astype(jnp.float32)).astype(jnp.bfloat16)
    own = lax.dynamic_slice_in_dim(joined, upper * half_slots, half_slots, 1)
    results = across(own).reshape(experts * capacity, columns)
    routed_rows = jnp.dot(
        combiner,
        results.astype(jnp.float32),
        precision=lax.Precision.HIGHEST,
        preferred_element_type=jnp.float32,
    ).astype(jnp.bfloat16)
    return (mixer_rows, routed_rows)


def _xor(value, mask):
    out, bit = value, 1
    while bit <= mask:
        if mask & bit:
            out = out + bit - 2 * bit * lax.rem(lax.div(value, bit), 2)
        bit *= 2
    return out


def _iota(shape, dim):
    return lax.broadcasted_iota(jnp.int32, shape, dim)


def _dot(a, b):
    return jnp.dot(a, b, preferred_element_type=jnp.float32)


def step_kernel(
    chips,
    cap,
    subs,
    pieces,
    halo,
    value_hbm,
    gate_hbm,
    taps_hbm,
    gain_hbm,
    wo_hbm,
    rows_hbm,
    egain_hbm,
    routes_hbm,
    rw_hbm,
    wg_hbm,
    wu_hbm,
    wd_hbm,
    mixer_ref,
    routed_ref,
    value_ref,
    gate_ref,
    taps_ref,
    gain_ref,
    rows_ref,
    egain_ref,
    routes_t_ref,
    rw_t_ref,
    wo,
    wg,
    wu,
    wd,
    normed,
    picked,
    block,
    hid,
    part,
    pair_in,
    cross_out,
    cross_in,
    back_out,
    results,
    near_out,
    near_res,
    q_out,
    q_in,
    combs,
    acc,
    glu,
    halo_out,
    halo_in,
    conv,
    w_sem,
    in_sem,
    far_recv,
    near_recv,
    xf_recv,
    cf_recv,
    cw_recv,
    r1_recv,
    r2_recv,
    r3_recv,
    r4_recv,
    q_recv,
    ag_recv,
    halo_recv,
    sent,
):
    f32, bf16 = jnp.float32, jnp.bfloat16
    ep = lax.axis_index("ep")
    x = lax.axis_index("tp")
    n_ep = 2 * chips
    z, c = lax.div(ep, 2), lax.rem(ep, 2)
    width = block.shape[-1]
    tokens = rows_ref.shape[0]
    length, local = value_ref.shape
    cols = local // LANES
    ntaps = taps_ref.shape[0]
    few = cap // subs
    split_from = max(1, chips // 2)
    far = list(range(split_from, chips))
    near = list(range(1, split_from))
    swap = 1 - lax.rem(z + lax.div(z, 2), 2)
    peers = [_xor(z, k) for k in range(chips)]
    for k in far:
        peers[k] = peers[k] + swap * (1 - 2 * lax.rem(peers[k], 2))

    def dev(zd, cd, xd):
        return {"ep": zd * 2 + cd, "tp": xd}

    def remote(src, dst, send, recv, to):
        return pltpu.make_async_remote_copy(
            src_ref=src, dst_ref=dst, send_sem=send, recv_sem=recv, device_id=to, device_id_type=MESH
        )

    to_send = {
        name: sent.at[i]
        for i, name in enumerate(["disp", "core", "pair", "cross", "back", "ag", "q", "halo"])
    }
    wing = lax.rem(z, chips // 2)
    core_peer = dev(z, 1 - c, x)
    plane_peer = dev(z, c, 1 - x)
    after = {"ep": lax.rem(ep + 1, n_ep), "tp": x}
    prior = {"ep": lax.rem(ep + n_ep - 1, n_ep), "tp": x}
    barrier = pltpu.get_barrier_semaphore()
    greeted = [core_peer, plane_peer, after, prior] + [dev(peers[k], c, x) for k in range(1, chips)]
    for to in greeted:
        pl.semaphore_signal(barrier, inc=1, device_id=to, device_id_type=MESH)

    inputs = [
        (rows_hbm, rows_ref),
        (routes_hbm, routes_t_ref),
        (rw_hbm, rw_t_ref),
        (egain_hbm, egain_ref),
        (value_hbm, value_ref),
        (gate_hbm, gate_ref),
        (taps_hbm, taps_ref),
        (gain_hbm, gain_ref),
    ]
    inputs = [pltpu.make_async_copy(a, b, in_sem.at[i]) for i, (a, b) in enumerate(inputs)]
    weights = [
        pltpu.make_async_copy(wg_hbm.at[0], wg, w_sem.at[0]),
        pltpu.make_async_copy(wu_hbm.at[0], wu, w_sem.at[1]),
        pltpu.make_async_copy(wd_hbm.at[0], wd, w_sem.at[2]),
        pltpu.make_async_copy(wo_hbm, wo, w_sem.at[3]),
    ]
    for copy in inputs:
        copy.start()
    for copy in inputs[:4]:
        copy.wait()
    erows = -(-chips // 8) * 8
    r0t, r1t = routes_t_ref[0:1, :], routes_t_ref[1:2, :]
    eid = _iota((erows, tokens), 0)
    hits_t = (r0t == eid) | (r1t == eid)
    earlier_t = (_iota((tokens, tokens), 0) < _iota((tokens, tokens), 1)).astype(f32)
    place_t = _dot(hits_t.astype(f32).astype(bf16), earlier_t.astype(bf16))
    slot_t = jnp.where(hits_t, place_t, -1.0).astype(jnp.int32)

    rows = rows_ref[...].astype(f32)
    scale = lax.rsqrt(jnp.mean(rows * rows, axis=-1, keepdims=True) + eps)
    both = (rows * scale * egain_ref[...]).astype(bf16)
    normed[0] = both[:, :width]
    normed[1] = both[:, width:]

    slots = _iota((cap, tokens), 0)

    def pick(k):
        row = jnp.sum(jnp.where(eid == peers[k], slot_t, 0), axis=0, keepdims=True)
        return (slots == row).astype(f32).astype(bf16)

    def cut(s):
        return slice(s * few, (s + 1) * few)

    for k in far:
        rows_k = _dot(pick(k), normed[x]).astype(bf16)
        for s in range(subs):
            picked[k, 0, s] = rows_k[cut(s)]
    for copy in inputs[4:]:
        copy.wait()
    for copy in weights:
        copy.start()
    last = slice(length - halo, length)
    gated = value_ref[last, :].astype(f32) * jax.nn.sigmoid(gate_ref[last, :].astype(f32))
    halo_out[...] = gated.astype(bf16)

    pl.semaphore_wait(barrier, len(greeted))
    halo_copy = remote(halo_out, halo_in, to_send["halo"], halo_recv.at[0], after)
    halo_copy.start()

    def far_copy(k, s, at):
        return remote(
            picked.at[k, 0, s],
            block.at[at, x, s, c],
            to_send["disp"],
            far_recv.at[lax.rem(at, chips // 2), s],
            dev(peers[k], c, x),
        )

    def near_dispatch(k, at):
        return remote(
            picked.at[k],
            block.at[at, :, :, c],
            to_send["disp"],
            near_recv.at[k - 1],
            dev(peers[k], c, x),
        )

    def core_copy(k, h, s, core):
        here = block.at[peers[k], h, s, core]
        return remote(here, here, to_send["core"], cf_recv.at[k - split_from, h, s], core_peer)

    def core_copies(k, core):
        here = block.at[peers[k], :, :, core]
        return remote(here, here, to_send["core"], cw_recv.at[k], core_peer)

    def plane_copy(k, h, s):
        here = block.at[peers[k], h, s, c]
        return remote(here, here, to_send["cross"], xf_recv.at[k - split_from, s], plane_peer)

    def from_core(k, h, s):
        core_copy(k, h, s, 1 - c).wait_recv()

    def slot_of_pair(k, s):
        return k if k < split_from else split_from + (k - split_from) * subs + s

    def pair_copy(k, o, s, n):
        h = x if o else 1 - x
        span = pl.ds(s * few, n)
        return remote(
            part.at[k, 1 - c, h, span],
            pair_in.at[k, h, span],
            to_send["pair"],
            r1_recv.at[slot_of_pair(k, s), o],
            core_peer,
        )

    def cross_copy(k, s, n):
        span = pl.ds(s * few, n)
        return remote(
            cross_out.at[k, span],
            cross_in.at[k, span],
            to_send["cross"],
            r2_recv.at[k - split_from, s],
            plane_peer,
        )

    def back_copy(k, s, n, at):
        span = pl.ds(s * few, n)
        return remote(
            back_out.at[k, span],
            results.at[at, span],
            to_send["back"],
            r3_recv.at[lax.rem(at, chips // 2), s],
            dev(peers[k], c, x),
        )

    def feed_forward(k, s, n, between=None, after_half=None):
        count = n // few
        zs = peers[k]
        a0 = block[zs, 0, s : s + count].reshape(2 * n, width)
        a1 = block[zs, 1, s : s + count].reshape(2 * n, width)
        units = hid.shape[1]
        step = min(units, 256)
        for j in range(0, units, step):
            gate = _dot(a0, wg[:width, j : j + step]) + _dot(a1, wg[width:, j : j + step])
            up = _dot(a0, wu[:width, j : j + step]) + _dot(a1, wu[width:, j : j + step])
            hid[: 2 * n, j : j + step] = (gate * jax.nn.sigmoid(gate) * up).astype(bf16)
        if between:
            between()
        h_all = hid[: 2 * n, :]
        for o in range(2):
            if o and after_half:
                after_half()
            h = x if o else 1 - x
            for j in range(0, width, step):
                at = pl.ds(pl.multiple_of(h * width + j, step), step)
                out = _dot(h_all, wd[:, at]).astype(bf16)
                for i in range(count):
                    for core in range(2):
                        r = (2 * i + core) * few
                        part[k, core, h, cut(s + i), j : j + step] = out[r : r + few]
            pair_copy(k, o, s, n).start()

    def pair_sum(k, s, n, wait=True):
        if wait:
            pair_copy(k, 0, s, n).wait_recv()
        span = slice(s * few, s * few + n)
        total = part[k, c, 1 - x, span].astype(f32) + pair_in[k, 1 - x, span].astype(f32)
        cross_out[k, span] = total.astype(bf16)
        cross_copy(k, s, n).start()

    def plane_sum(k, s, n, wait=True):
        if wait:
            pair_copy(k, 1, s, n).wait_recv()
        cross_copy(k, s, n).wait_recv()
        span = slice(s * few, s * few + n)
        total = (
            part[k, c, x, span].astype(f32)
            + pair_in[k, x, span].astype(f32)
            + cross_in[k, span].astype(f32)
        )
        back_out[k, span] = total.astype(bf16)
        back_copy(k, s, n, z).start()

    piece = width // 2

    def near_copy(k, o, j=0):
        part_cols = pl.ds(0, width) if o else pl.ds(j * piece, piece)
        return remote(
            near_out.at[k, o, :, part_cols],
            near_res.at[k, o, :, part_cols],
            to_send["back"],
            r4_recv.at[k - 1, 2 if o else j],
            dev(peers[k], c, x),
        )

    def near_sum(k, o):
        pair_copy(k, o, 0, cap).wait_recv()
        h = x if o else 1 - x
        total = part[k, c, h].astype(f32) + pair_in[k, h].astype(f32)
        near_out[k, o] = total.astype(bf16)
        if k:
            for j in range(1 if o else 2):
                near_copy(k, o, j).start()

    def q_copy(j):
        part_cols = pl.ds(j * piece, piece)
        return remote(
            q_out.at[:, part_cols], q_in.at[:, part_cols], to_send["q"], q_recv.at[j], plane_peer
        )

    def lend(j):
        at = slice(j * piece, (j + 1) * piece)
        total = weighed(0, near_out[0, 0, :, at])
        for k in near:
            near_copy(k, 0, j).wait_recv()
            total = total + weighed(k, near_res[k, 0, :, at])
        q_out[:, at] = total.astype(bf16)
        q_copy(j).start()

    def keep():
        total = weighed(0, near_out[0, 1])
        for k in near:
            near_copy(k, 1).wait_recv()
            total = total + weighed(k, near_res[k, 1])
        acc[...] = total

    def pair_sums(k):
        pair_copy(k, 0, 0, cap).wait_recv()
        for s in range(subs):
            pair_sum(k, s, few, False)

    def plane_sums(k):
        pair_copy(k, 1, 0, cap).wait_recv()
        for s in range(subs):
            plane_sum(k, s, few, False)

    def send_far():
        for s in range(subs):
            for k in far:
                far_copy(k, s, z).start()

    def far_in(k, s):
        far_copy(k, s, peers[k]).wait_recv()
        plane_copy(k, x, s).start()
        core_copy(k, x, s, c).start()

    def far_over(k, s):
        plane_copy(k, 1 - x, s).wait_recv()
        core_copy(k, 1 - x, s, c).start()

    def near_in(k):
        near_dispatch(k, peers[k]).wait_recv()
        core_copies(k, c).start()

    def from_cores(k):
        if k < split_from:
            core_copies(k, 1 - c).wait_recv()
        else:
            for h in range(2):
                for s in range(subs):
                    from_core(k, h, s)

    def weighed(k, found):
        return _dot(combs[k, 0], found) + _dot(combs[k, 1], found)

    rows_per = length // pieces
    tile = 64 if rows_per % 64 == 0 else rows_per

    early = min(pieces, 4)
    groups = [(p, p + 1) for p in range(1, early)]
    groups += [(p, min(p + 2, pieces)) for p in range(early, pieces, 2)] + [(0, 1)]
    gathered = set()

    def gather_copy(g, who):
        lo, hi = groups[g]
        rows_g = conv.at[who, pl.ds(lo * rows_per, (hi - lo) * rows_per)]
        return remote(rows_g, rows_g, to_send["ag"], ag_recv.at[g], plane_peer)

    def gather(lo, hi):
        for g in range(lo, hi):
            gather_copy(g, x).start()

    def convolve(lo, hi, send=False):
        def conv_tile(r, carry):
            r0 = pl.multiple_of(r * tile, tile)
            for i in range(cols):
                total = jnp.zeros((tile, LANES), f32)
                for k in range(ntaps):
                    total = (
                        total
                        + taps_ref[k : k + 1, i * LANES : (i + 1) * LANES]
                        * glu[i, pl.ds(r0 + (k + halo - ntaps + 1), tile), :]
                    )
                conv[x, pl.ds(r0, tile), i * LANES : (i + 1) * LANES] = total.astype(bf16)
            if send:
                rows_r = conv.at[x, pl.ds(r0, tile)]
                remote(rows_r, rows_r, to_send["ag"], ag_recv.at[r - 1], plane_peer).start()
            return carry

        per = rows_per // tile
        send = send and per == 1
        lax.fori_loop(lo * per, hi * per, conv_tile, 0)
        return send

    def mix(lo, hi):
        for g, (first, last) in enumerate(groups):
            if g not in gathered and first < hi and last > lo:
                gather_copy(g, 1 - x).wait_recv()
                gathered.add(g)
        here = slice(lo * rows_per, hi * rows_per)
        first, second = conv[0, here, :].astype(f32), conv[1, here, :].astype(f32)
        count = 2 * local
        mean = (
            jnp.sum(first, axis=-1, keepdims=True) + jnp.sum(second, axis=-1, keepdims=True)
        ) / count
        first, second = first - mean, second - mean
        var = (
            jnp.sum(first * first, axis=-1, keepdims=True)
            + jnp.sum(second * second, axis=-1, keepdims=True)
        ) / count
        scale = lax.rsqrt(var + eps)
        first = first * scale * gain_ref[:, :local]
        second = second * scale * gain_ref[:, local:]
        first = (first * jax.nn.sigmoid(first)).astype(bf16)
        second = (second * jax.nn.sigmoid(second)).astype(bf16)
        mixer_ref[here, :] = (_dot(first, wo[:local, :]) + _dot(second, wo[local:, :])).astype(bf16)

    def combine(k):
        return acc[...] + weighed(k, results[peers[k]])

    def returned(k, n):
        for s in range(subs):
            back_copy(k, s, n, peers[k]).wait_recv()

    send_far()
    for k in near:
        rows_k = [_dot(pick(k), normed[h]).astype(bf16) for h in range(2)]
        for h in range(2):
            for s in range(subs):
                picked[k, h, s] = rows_k[h][cut(s)]
        near_dispatch(k, z).start()
    for h in range(2):
        rows_0 = _dot(pick(0), normed[h]).astype(bf16)
        for s in range(subs):
            block[z, h, s, c] = rows_0[cut(s)]
    core_copies(0, c).start()
    kept = slice(0, length - halo)
    for i in range(cols):
        at = slice(i * LANES, (i + 1) * LANES)
        gated = value_ref[kept, at].astype(f32) * jax.nn.sigmoid(gate_ref[kept, at].astype(f32))
        glu[i, halo:length, :] = gated.astype(bf16).astype(f32)
        glu[i, length:, :] = halo_out[:, at].astype(f32)
    if not convolve(1, early, True):
        gather(0, early - 1)
    convolve(early, pieces)
    mid_far, last_far = far[:-1], far[-1]
    units = [(k, s) for k in mid_far for s in range(subs)]
    lane = _iota((tokens, LANES), 1)
    index = _iota((8, tokens), 0)
    rows_named = jnp.where(index == 0, r0t, 0).astype(f32) + jnp.where(index == 1, r1t, 0).astype(f32)
    for j in range(2):
        rows_named = rows_named + jnp.where(index == 2 + j, rw_t_ref[j : j + 1, :], 0.0)
    named = jnp.transpose(rows_named)
    r0, r1 = (named[:, j : j + 1].astype(jnp.int32) for j in range(2))
    hits = ((r0 == lane) | (r1 == lane)).astype(f32).astype(bf16)
    earlier = (_iota((tokens, tokens), 1) < _iota((tokens, tokens), 0)).astype(f32).astype(bf16)
    place = _dot(earlier, hits)
    slot_of = _iota((tokens, cap), 1)
    places = [
        jnp.sum(jnp.where(lane == r, place, 0.0), axis=1, keepdims=True).astype(jnp.int32)
        for r in (r0, r1)
    ]
    for k in range(chips):
        comb = jnp.zeros((tokens, cap), f32)
        for j, r in enumerate((r0, r1)):
            mine = jnp.where(r == peers[k], places[j], -1)
            comb = comb + jnp.where(slot_of == mine, named[:, 2 + j : 3 + j], 0.0)
        head = comb.astype(bf16)
        combs[k, 0] = head
        combs[k, 1] = (comb - head.astype(f32)).astype(bf16)


    halo_copy.wait_recv()
    before = jnp.where(ep > 0, halo_in[...].astype(f32), 0.0)
    for i in range(cols):
        glu[i, :halo, :] = before[:, i * LANES : (i + 1) * LANES]
    convolve(0, 1)
    for copy in weights[:3]:
        copy.wait()
    from_cores(0)
    feed_forward(0, 0, cap, lambda: far_in(*units[0]))
    far_over(*units[0])
    for unit in units[1:]:
        far_in(*unit)
    later = min(len(groups), early)
    gather(early - 1, later)
    for o in range(2):
        near_sum(0, o)
    for h in range(2):
        from_core(units[0][0], h, units[0][1])
    feed_forward(*units[0], few, lambda: far_in(last_far, 0))

    def near_ins():
        for k in near:
            near_in(k)

    def last_ins():
        for s in range(1, subs):
            far_in(last_far, s)

    if len(units) == 1:
        near_ins()
        last_ins()
    for i in range(1, len(units)):
        far_over(*units[i])
        pair_sum(*units[i - 1], few)
        for h in range(2):
            from_core(units[i][0], h, units[i][1])
        only = i == 1
        feed_forward(*units[i], few, near_ins if only else None, last_ins if only else None)
    far_over(last_far, 0)
    for k in near:
        from_cores(k)

    def first_back():
        pair_sum(*units[-1], few)
        plane_sum(*units[0], few)

    for k in near:
        feed_forward(k, 0, cap, first_back if k == near[0] else None)
    gather(later, len(groups) - 1)
    for s in range(1, subs):
        far_over(last_far, s)

    def near_sums(o):
        for k in near:
            near_sum(k, o)


    for s in range(subs):
        for h in range(2):
            from_core(last_far, h, s)
        if s == 0:
            feed_forward(last_far, s, few, lambda: near_sums(0), lambda: near_sums(1))
        else:
            for unit in units[1:] if s == 1 else []:
                plane_sum(*unit, few)
            feed_forward(last_far, s, few, lambda: pair_sum(last_far, s - 1, few))
    pair_sum(last_far, subs - 1, few)
    gather(len(groups) - 1, len(groups))
    weights[3].wait()
    group = 2 if pieces % 2 == 0 else 1
    mix(group, 2 * group)
    plane_sum(last_far, 0, few)
    for p in range(2 * group, pieces, group):
        mix(p, p + group)

    def lend_all():
        lend(0)
        lend(1)

    pl.when(swap == 0)(lend_all)
    pl.when(swap == 1)(lambda: lend(0))
    for s in range(1, subs):
        plane_sum(last_far, s, few)
    pl.when(swap == 1)(lambda: lend(1))
    mix(0, group)
    keep()
    for k in far[:-1]:
        returned(k, few)
        acc[...] = combine(k)
    for j in range(2):
        q_copy(j).wait_recv()
    acc[...] = acc[...] + q_in[...].astype(f32)
    returned(far[-1], few)
    routed_ref[...] = combine(far[-1]).astype(bf16)

    half = block.at[pl.ds(0, chips // 2)]
    for name, ref in (
        ("disp", block.at[0]),
        ("core", half),
        ("pair", half),
        ("cross", block.at[0]),
        ("back", block.at[0]),
        ("ag", conv.at[0]),
        ("q", q_out),
        ("halo", halo_out),
    ):
        remote(ref, ref, to_send[name], halo_recv.at[0], core_peer).wait_send()


def store_kernel(mixer_ref, routed_ref, mixer_hbm, routed_hbm, sem):
    copies = [
        pltpu.make_async_copy(mixer_ref, mixer_hbm, sem.at[0]),
        pltpu.make_async_copy(routed_ref, routed_hbm, sem.at[1]),
    ]
    for copy in copies:
        copy.start()
    for copy in copies:
        copy.wait()


def one_kernel(
    value_in,
    gate_in,
    conv_taps,
    chan_gain,
    out_weight,
    second_rows,
    expert_gain,
    routes,
    route_weights,
    gate_w,
    up_w,
    down_w,
):
    chips = lax.axis_size("ep") // 2
    tokens, model = second_rows.shape
    top = routes.shape[1]
    width = model // 2
    cap = 2 * max(1, min(tokens // 2, 3 * tokens * top // (4 * chips)))
    subs = 2 if cap % 32 == 0 else 1
    few = cap // subs
    length, local = value_in.shape
    units = gate_w.shape[2]
    halo = -(-(conv_taps.shape[0] - 1) // 16) * 16
    pieces = 8 if length % 128 == 0 and length // 8 > halo else 1
    bf16, f32 = jnp.bfloat16, jnp.float32
    vmem = pl.BlockSpec(memory_space=pltpu.VMEM)
    hbm = pl.BlockSpec(memory_space=pltpu.HBM)
    dma = pltpu.SemaphoreType.DMA
    scratch = [
        pltpu.VMEM(value_in.shape, bf16),
        pltpu.VMEM(gate_in.shape, bf16),
        pltpu.VMEM(conv_taps.shape, f32),
        pltpu.VMEM((1, chan_gain.shape[0]), f32),
        pltpu.VMEM(second_rows.shape, bf16),
        pltpu.VMEM((1, model), f32),
        pltpu.VMEM((top, tokens), jnp.int32),
        pltpu.VMEM((top, tokens), f32),
        pltpu.VMEM(out_weight.shape, bf16),
        pltpu.VMEM(gate_w.shape[1:], bf16),
        pltpu.VMEM(up_w.shape[1:], bf16),
        pltpu.VMEM(down_w.shape[1:], bf16),
        pltpu.VMEM((2, tokens, width), bf16),
        pltpu.VMEM((chips, 2, subs, few, width), bf16),
        pltpu.VMEM((chips, 2, subs, 2, few, width), bf16),
        pltpu.VMEM((2 * cap, units), bf16),
        pltpu.VMEM((chips, 2, 2, cap, width), bf16),
        pltpu.VMEM((chips, 2, cap, width), bf16),
        pltpu.VMEM((chips, cap, width), bf16),
        pltpu.VMEM((chips, cap, width), bf16),
        pltpu.VMEM((chips, cap, width), bf16),
        pltpu.VMEM((chips, cap, width), bf16),
        pltpu.VMEM((chips // 2, 2, cap, width), bf16),
        pltpu.VMEM((chips // 2, 2, cap, width), bf16),
        pltpu.VMEM((tokens, width), bf16),
        pltpu.VMEM((tokens, width), bf16),
        pltpu.VMEM((chips, 2, tokens, cap), bf16),
        pltpu.VMEM((tokens, width), f32),
        pltpu.VMEM((local // LANES, halo + length, LANES), f32),
        pltpu.VMEM((halo, local), bf16),
        pltpu.VMEM((halo, local), bf16),
        pltpu.VMEM((2, length, local), bf16),
        dma((4,)),
        dma((8,)),
        dma((chips // 2, subs)),
        dma((chips // 2 - 1,)),
        dma((chips // 2, subs)),
        dma((chips // 2, 2, subs)),
        dma((chips // 2,)),
        dma((chips // 2 + chips // 2 * subs, 2)),
        dma((chips // 2, subs)),
        dma((chips // 2, subs)),
        dma((chips // 2 - 1, 3)),
        dma((2,)),
        dma((min(pieces, 4) + (pieces - min(pieces, 4) + 1) // 2,)),
        dma((1,)),
        dma((8,)),
    ]
    outs = pl.pallas_call(
        functools.partial(step_kernel, chips, cap, subs, pieces, halo),
        out_shape=(
            jax.ShapeDtypeStruct((length, out_weight.shape[1]), bf16),
            jax.ShapeDtypeStruct((tokens, width), bf16),
        ),
        in_specs=[hbm] * 12,
        out_specs=(vmem, vmem),
        scratch_shapes=scratch,
        compiler_params=pltpu.CompilerParams(
            collective_id=0, has_side_effects=True, vmem_limit_bytes=40 * 1024 * 1024
        ),
    )(
        *(
            pltpu.with_memory_space_constraint(value, pltpu.HBM)
            for value in (
                value_in,
                gate_in,
                conv_taps,
                chan_gain.reshape(1, -1),
                out_weight,
                second_rows,
                expert_gain.reshape(1, -1),
                routes.T,
                route_weights.T,
                gate_w,
                up_w,
                down_w,
            )
        )
    )
    return pl.pallas_call(
        store_kernel,
        out_shape=tuple(jax.ShapeDtypeStruct(out.shape, out.dtype) for out in outs),
        in_specs=[vmem] * 2,
        out_specs=(pl.BlockSpec(memory_space=pl.ANY),) * 2,
        scratch_shapes=[dma((2,))],
        compiler_params=pltpu.CompilerParams(vmem_limit_bytes=1024 * 1024),
    )(*outs)


def solution(mesh):
    chips = mesh.shape["ep"] // 2
    paired = mesh.shape["tp"] == 2 and chips == 4
    placed = (
        P(("grp", "ep"), "tp"),
        P(("grp", "ep"), "tp"),
        P(None, "tp"),
        P(),
        P(None, "tp"),
        P(("grp", "ep"), None),
        P(),
        P(("grp", "ep"), None),
        P(("grp", "ep"), None),
        P("ep", None, "tp"),
        P("ep", None, "tp"),
        P("ep", "tp", None),
    )
    return jax.shard_map(
        one_kernel if paired else on_device,
        mesh=mesh,
        in_specs=placed,
        out_specs=(P(("grp", "ep"), "tp"), P(("grp", "ep"), "tp")),
        check_vma=False,
    )
```

```python
import functools

import jax
import jax.numpy as jnp
from jax import lax
from jax.experimental import pallas as pl
from jax.experimental.pallas import tpu as pltpu
from jax.sharding import PartitionSpec as P

eps = 1e-06
LANES = 128
MESH = pl.DeviceIdType.MESH


def partner_2(value, axis, bit):
    return lax.ppermute(value, axis, [(i, i ^ 1 << bit) for i in range(lax.axis_size(axis))])


def shifted(value, axis, by):
    devices = lax.axis_size(axis)
    pairs = [(i, i + by) for i in range(devices) if 0 <= i + by < devices]
    return lax.ppermute(value, axis, pairs)


def partner(block):
    return partner_2(block, "ep", 0)


def across(block):
    return lax.all_to_all(block, "ep", split_axis=0, concat_axis=0, tiled=True)


def on_device(
    value_in,
    gate_in,
    conv_taps,
    chan_gain,
    out_weight,
    second_rows,
    expert_gain,
    routes,
    route_weights,
    gate_w,
    up_w,
    down_w,
):
    taps = conv_taps.shape[0]
    glu = (value_in.astype(jnp.float32) * jax.nn.sigmoid(gate_in.astype(jnp.float32))).astype(
        jnp.bfloat16
    )
    length = glu.shape[0]
    before = shifted(glu[length - taps + 1 :], "ep", 1)
    padded = jnp.concatenate([before, glu], axis=0).astype(jnp.float32)
    total = jnp.zeros(glu.shape, jnp.float32)
    for offset in range(taps):
        total = total + conv_taps[offset][None, :] * padded[offset : offset + length]
    convolved = total.astype(jnp.bfloat16)
    channels = lax.all_gather(convolved, "tp", axis=1, tiled=True)
    values = channels.astype(jnp.float32)
    centered = values - jnp.mean(values, axis=-1, keepdims=True)
    scaled = (
        centered
        * lax.rsqrt(jnp.mean(centered * centered, axis=-1, keepdims=True) + eps)
        * chan_gain
    )
    activated = jax.nn.silu(scaled).astype(jnp.bfloat16)
    mixer_rows = jnp.dot(activated, out_weight, preferred_element_type=jnp.float32).astype(
        jnp.bfloat16
    )
    n_ep = lax.axis_size("ep")
    experts = n_ep // 2
    tokens = second_rows.shape[0]
    top = routes.shape[1]
    width = second_rows.shape[1]
    capacity = 2 * max(1, min(tokens // 2, 3 * tokens * top // (4 * experts)))
    half_slots = capacity // 2
    rows = second_rows.astype(jnp.float32)
    normed = (
        rows * lax.rsqrt(jnp.mean(rows * rows, axis=-1, keepdims=True) + eps) * expert_gain
    ).astype(jnp.bfloat16)
    chosen = routes.reshape(-1)
    hits = (chosen[:, None] == jnp.arange(experts, dtype=jnp.int32)[None, :]).astype(jnp.int32)
    place = jnp.sum((jnp.cumsum(hits, axis=0) - 1) * hits, axis=1)
    target = (chosen * capacity + place).reshape(tokens, top)
    slots = jnp.arange(experts * capacity, dtype=jnp.int32)
    matches = target[:, :, None] == slots[None, None, :]
    picker = jnp.any(matches, axis=1).astype(jnp.bfloat16)
    outgoing = jnp.dot(picker.T, normed, preferred_element_type=jnp.float32).astype(jnp.bfloat16)
    combiner = jnp.sum(jnp.where(matches, route_weights[:, :, None], 0.0), axis=1)
    upper = lax.axis_index("ep") % 2
    arrived = across(outgoing.reshape(n_ep, half_slots, width))
    other = partner(arrived)
    first = jnp.where(upper == 0, arrived, other)
    second = jnp.where(upper == 0, other, arrived)
    incoming = jnp.concatenate([first, second], axis=1)
    block_rows = incoming.reshape(n_ep * capacity, width)
    gate = jnp.dot(block_rows, gate_w[0], preferred_element_type=jnp.float32)
    lifted = jnp.dot(block_rows, up_w[0], preferred_element_type=jnp.float32)
    hidden = (jax.nn.silu(gate) * lifted).astype(jnp.bfloat16)
    partial_value = jnp.dot(hidden, down_w[0], preferred_element_type=jnp.float32)
    half_sums = lax.psum_scatter(
        partial_value.astype(jnp.bfloat16), "tp", scatter_dimension=1, tiled=True
    )
    columns = half_sums.shape[1]
    half_sums = half_sums.reshape(n_ep, capacity, columns)
    other_sums = partner(half_sums)
    joined = (half_sums.astype(jnp.float32) + other_sums.astype(jnp.float32)).astype(jnp.bfloat16)
    own = lax.dynamic_slice_in_dim(joined, upper * half_slots, half_slots, 1)
    results = across(own).reshape(experts * capacity, columns)
    routed_rows = jnp.dot(
        combiner,
        results.astype(jnp.float32),
        precision=lax.Precision.HIGHEST,
        preferred_element_type=jnp.float32,
    ).astype(jnp.bfloat16)
    return (mixer_rows, routed_rows)


def _xor(value, mask):
    out, bit = value, 1
    while bit <= mask:
        if mask & bit:
            out = out + bit - 2 * bit * lax.rem(lax.div(value, bit), 2)
        bit *= 2
    return out


def _iota(shape, dim):
    return lax.broadcasted_iota(jnp.int32, shape, dim)


def _dot(a, b):
    return jnp.dot(a, b, preferred_element_type=jnp.float32)


def step_kernel(
    chips,
    cap,
    subs,
    pieces,
    halo,
    value_hbm,
    gate_hbm,
    taps_hbm,
    gain_hbm,
    wo_hbm,
    rows_hbm,
    egain_hbm,
    routes_hbm,
    rw_hbm,
    wg_hbm,
    wu_hbm,
    wd_hbm,
    mixer_ref,
    routed_ref,
    value_ref,
    gate_ref,
    taps_ref,
    gain_ref,
    rows_ref,
    egain_ref,
    routes_t_ref,
    rw_t_ref,
    wo,
    wg,
    wu,
    wd,
    normed,
    picked,
    block,
    hid,
    part,
    pair_in,
    cross_out,
    cross_in,
    back_out,
    results,
    near_out,
    near_res,
    q_out,
    q_in,
    combs,
    acc,
    glu,
    halo_out,
    halo_in,
    conv,
    w_sem,
    in_sem,
    far_recv,
    near_recv,
    xf_recv,
    cf_recv,
    cw_recv,
    r1_recv,
    r2_recv,
    r3_recv,
    r4_recv,
    q_recv,
    ag_recv,
    halo_recv,
    sent,
):
    f32, bf16 = jnp.float32, jnp.bfloat16
    ep = lax.axis_index("ep")
    x = lax.axis_index("tp")
    n_ep = 2 * chips
    z, c = lax.div(ep, 2), lax.rem(ep, 2)
    width = block.shape[-1]
    tokens = rows_ref.shape[0]
    length, local = value_ref.shape
    cols = local // LANES
    ntaps = taps_ref.shape[0]
    few = cap // subs
    split_from = max(1, chips // 2)
    far = list(range(split_from, chips))
    near = list(range(1, split_from))
    swap = 1 - lax.rem(z + lax.div(z, 2), 2)
    peers = [_xor(z, k) for k in range(chips)]
    for k in far:
        peers[k] = peers[k] + swap * (1 - 2 * lax.rem(peers[k], 2))

    def dev(zd, cd, xd):
        return {"ep": zd * 2 + cd, "tp": xd}

    def remote(src, dst, send, recv, to):
        return pltpu.make_async_remote_copy(
            src_ref=src, dst_ref=dst, send_sem=send, recv_sem=recv, device_id=to, device_id_type=MESH
        )

    to_send = {
        name: sent.at[i]
        for i, name in enumerate(["disp", "core", "pair", "cross", "back", "ag", "q", "halo"])
    }
    wing = lax.rem(z, chips // 2)
    core_peer = dev(z, 1 - c, x)
    plane_peer = dev(z, c, 1 - x)
    after = {"ep": lax.rem(ep + 1, n_ep), "tp": x}
    prior = {"ep": lax.rem(ep + n_ep - 1, n_ep), "tp": x}
    barrier = pltpu.get_barrier_semaphore()
    greeted = [core_peer, plane_peer, after, prior] + [dev(peers[k], c, x) for k in range(1, chips)]
    for to in greeted:
        pl.semaphore_signal(barrier, inc=1, device_id=to, device_id_type=MESH)

    inputs = [
        (routes_hbm, routes_t_ref),
        (rows_hbm, rows_ref),
        (egain_hbm, egain_ref),
        (rw_hbm, rw_t_ref),
        (value_hbm, value_ref),
        (gate_hbm, gate_ref),
        (taps_hbm, taps_ref),
        (gain_hbm, gain_ref),
    ]
    inputs = [pltpu.make_async_copy(a, b, in_sem.at[i]) for i, (a, b) in enumerate(inputs)]
    weights = [
        pltpu.make_async_copy(wg_hbm.at[0], wg, w_sem.at[0]),
        pltpu.make_async_copy(wu_hbm.at[0], wu, w_sem.at[1]),
        pltpu.make_async_copy(wd_hbm.at[0], wd, w_sem.at[2]),
        pltpu.make_async_copy(wo_hbm, wo, w_sem.at[3]),
    ]
    for copy in inputs:
        copy.start()
    inputs[0].wait()
    erows = -(-chips // 8) * 8
    r0t, r1t = routes_t_ref[0:1, :], routes_t_ref[1:2, :]
    eid = _iota((erows, tokens), 0)
    hits_t = (r0t == eid) | (r1t == eid)
    earlier_t = (_iota((tokens, tokens), 0) < _iota((tokens, tokens), 1)).astype(f32)
    place_t = _dot(hits_t.astype(f32).astype(bf16), earlier_t.astype(bf16))
    slot_t = jnp.where(hits_t, place_t, -1.0).astype(jnp.int32)

    slots = _iota((cap, tokens), 0)

    pickers = []
    for k in range(chips):
        row = jnp.sum(jnp.where(eid == peers[k], slot_t, 0), axis=0, keepdims=True)
        pickers.append((slots == row).astype(f32).astype(bf16))
    for copy in inputs[1:3]:
        copy.wait()
    rows = rows_ref[...].astype(f32)
    scale = lax.rsqrt(jnp.mean(rows * rows, axis=-1, keepdims=True) + eps)
    both = (rows * scale * egain_ref[...]).astype(bf16)
    normed[0] = both[:, :width]
    normed[1] = both[:, width:]

    def cut(s):
        return slice(s * few, (s + 1) * few)

    for k in far:
        rows_k = _dot(pickers[k], normed[x]).astype(bf16)
        for s in range(subs):
            picked[k, 0, s] = rows_k[cut(s)]
    for copy in inputs[3:]:
        copy.wait()
    for copy in weights:
        copy.start()
    last = slice(length - halo, length)
    gated = value_ref[last, :].astype(f32) * jax.nn.sigmoid(gate_ref[last, :].astype(f32))
    halo_out[...] = gated.astype(bf16)

    pl.semaphore_wait(barrier, len(greeted))
    halo_copy = remote(halo_out, halo_in, to_send["halo"], halo_recv.at[0], after)
    halo_copy.start()

    def far_copy(k, s, at):
        return remote(
            picked.at[k, 0, s],
            block.at[at, x, s, c],
            to_send["disp"],
            far_recv.at[lax.rem(at, chips // 2), s],
            dev(peers[k], c, x),
        )

    def near_dispatch(k, at):
        return remote(
            picked.at[k],
            block.at[at, :, :, c],
            to_send["disp"],
            near_recv.at[k - 1],
            dev(peers[k], c, x),
        )

    def core_copy(k, h, s, core):
        here = block.at[peers[k], h, s, core]
        return remote(here, here, to_send["core"], cf_recv.at[k - split_from, h, s], core_peer)

    def core_copies(k, core):
        here = block.at[peers[k], :, :, core]
        return remote(here, here, to_send["core"], cw_recv.at[k], core_peer)

    def plane_copy(k, h, s):
        here = block.at[peers[k], h, s, c]
        return remote(here, here, to_send["cross"], xf_recv.at[k - split_from, s], plane_peer)

    def from_core(k, h, s):
        core_copy(k, h, s, 1 - c).wait_recv()

    def slot_of_pair(k, s):
        return k if k < split_from else split_from + (k - split_from) * subs + s

    def pair_copy(k, o, s, n):
        h = x if o else 1 - x
        span = pl.ds(s * few, n)
        return remote(
            part.at[k, 1 - c, h, span],
            pair_in.at[k, h, span],
            to_send["pair"],
            r1_recv.at[slot_of_pair(k, s), o],
            core_peer,
        )

    def cross_copy(k, s, n):
        span = pl.ds(s * few, n)
        return remote(
            cross_out.at[k, span],
            cross_in.at[k, span],
            to_send["cross"],
            r2_recv.at[k - split_from, s],
            plane_peer,
        )

    def back_copy(k, s, n, at):
        span = pl.ds(s * few, n)
        return remote(
            back_out.at[k, span],
            results.at[at, span],
            to_send["back"],
            r3_recv.at[lax.rem(at, chips // 2), s],
            dev(peers[k], c, x),
        )

    def feed_forward(k, s, n, between=None, after_half=None):
        count = n // few
        zs = peers[k]
        a0 = block[zs, 0, s : s + count].reshape(2 * n, width)
        a1 = block[zs, 1, s : s + count].reshape(2 * n, width)
        units = hid.shape[1]
        step = min(units, 256)
        for j in range(0, units, step):
            gate = _dot(a0, wg[:width, j : j + step]) + _dot(a1, wg[width:, j : j + step])
            up = _dot(a0, wu[:width, j : j + step]) + _dot(a1, wu[width:, j : j + step])
            hid[: 2 * n, j : j + step] = (gate * jax.nn.sigmoid(gate) * up).astype(bf16)
        if between:
            between()
        h_all = hid[: 2 * n, :]
        for o in range(2):
            if o and after_half:
                after_half()
            h = x if o else 1 - x
            for j in range(0, width, step):
                at = pl.ds(pl.multiple_of(h * width + j, step), step)
                out = _dot(h_all, wd[:, at]).astype(bf16)
                for i in range(count):
                    for core in range(2):
                        r = (2 * i + core) * few
                        part[k, core, h, cut(s + i), j : j + step] = out[r : r + few]
            pair_copy(k, o, s, n).start()

    def pair_sum(k, s, n, wait=True):
        if wait:
            pair_copy(k, 0, s, n).wait_recv()
        span = slice(s * few, s * few + n)
        total = part[k, c, 1 - x, span].astype(f32) + pair_in[k, 1 - x, span].astype(f32)
        cross_out[k, span] = total.astype(bf16)
        cross_copy(k, s, n).start()

    def plane_sum(k, s, n, wait=True):
        if wait:
            pair_copy(k, 1, s, n).wait_recv()
        cross_copy(k, s, n).wait_recv()
        span = slice(s * few, s * few + n)
        total = (
            part[k, c, x, span].astype(f32)
            + pair_in[k, x, span].astype(f32)
            + cross_in[k, span].astype(f32)
        )
        back_out[k, span] = total.astype(bf16)
        back_copy(k, s, n, z).start()

    piece = width // 2

    def near_copy(k, o, j=0):
        part_cols = pl.ds(0, width) if o else pl.ds(j * piece, piece)
        return remote(
            near_out.at[k, o, :, part_cols],
            near_res.at[k, o, :, part_cols],
            to_send["back"],
            r4_recv.at[k - 1, 2 if o else j],
            dev(peers[k], c, x),
        )

    def near_sum(k, o):
        pair_copy(k, o, 0, cap).wait_recv()
        h = x if o else 1 - x
        total = part[k, c, h].astype(f32) + pair_in[k, h].astype(f32)
        near_out[k, o] = total.astype(bf16)
        if k:
            for j in range(1 if o else 2):
                near_copy(k, o, j).start()

    def q_copy(j):
        part_cols = pl.ds(j * piece, piece)
        return remote(
            q_out.at[:, part_cols], q_in.at[:, part_cols], to_send["q"], q_recv.at[j], plane_peer
        )

    def lend(j):
        at = slice(j * piece, (j + 1) * piece)
        total = weighed(0, near_out[0, 0, :, at])
        for k in near:
            near_copy(k, 0, j).wait_recv()
            total = total + weighed(k, near_res[k, 0, :, at])
        q_out[:, at] = total.astype(bf16)
        q_copy(j).start()

    def keep():
        total = weighed(0, near_out[0, 1])
        for k in near:
            near_copy(k, 1).wait_recv()
            total = total + weighed(k, near_res[k, 1])
        acc[...] = total

    def pair_sums(k):
        pair_copy(k, 0, 0, cap).wait_recv()
        for s in range(subs):
            pair_sum(k, s, few, False)

    def plane_sums(k):
        pair_copy(k, 1, 0, cap).wait_recv()
        for s in range(subs):
            plane_sum(k, s, few, False)

    def send_far():
        for s in range(subs):
            for k in far:
                far_copy(k, s, z).start()

    def far_in(k, s):
        far_copy(k, s, peers[k]).wait_recv()
        plane_copy(k, x, s).start()
        core_copy(k, x, s, c).start()

    def far_over(k, s):
        plane_copy(k, 1 - x, s).wait_recv()
        core_copy(k, 1 - x, s, c).start()

    def near_in(k):
        near_dispatch(k, peers[k]).wait_recv()
        core_copies(k, c).start()

    def from_cores(k):
        if k < split_from:
            core_copies(k, 1 - c).wait_recv()
        else:
            for h in range(2):
                for s in range(subs):
                    from_core(k, h, s)

    def weighed(k, found):
        return _dot(combs[k, 0], found) + _dot(combs[k, 1], found)

    rows_per = length // pieces
    tile = 64 if rows_per % 64 == 0 else rows_per

    early = min(pieces, 4)
    groups = [(p, p + 1) for p in range(1, early)]
    groups += [(p, min(p + 2, pieces)) for p in range(early, pieces, 2)] + [(0, 1)]
    gathered = set()

    def gather_copy(g, who):
        lo, hi = groups[g]
        rows_g = conv.at[who, pl.ds(lo * rows_per, (hi - lo) * rows_per)]
        return remote(rows_g, rows_g, to_send["ag"], ag_recv.at[g], plane_peer)

    def gather(lo, hi):
        for g in range(lo, hi):
            gather_copy(g, x).start()

    def convolve(lo, hi, send=False):
        def conv_tile(r, carry):
            r0 = pl.multiple_of(r * tile, tile)
            for i in range(cols):
                total = jnp.zeros((tile, LANES), f32)
                for k in range(ntaps):
                    total = (
                        total
                        + taps_ref[k : k + 1, i * LANES : (i + 1) * LANES]
                        * glu[i, pl.ds(r0 + (k + halo - ntaps + 1), tile), :]
                    )
                conv[x, pl.ds(r0, tile), i * LANES : (i + 1) * LANES] = total.astype(bf16)
            if send:
                rows_r = conv.at[x, pl.ds(r0, tile)]
                remote(rows_r, rows_r, to_send["ag"], ag_recv.at[r - 1], plane_peer).start()
            return carry

        per = rows_per // tile
        send = send and per == 1
        lax.fori_loop(lo * per, hi * per, conv_tile, 0)
        return send

    def mix(lo, hi):
        for g, (first, last) in enumerate(groups):
            if g not in gathered and first < hi and last > lo:
                gather_copy(g, 1 - x).wait_recv()
                gathered.add(g)
        here = slice(lo * rows_per, hi * rows_per)
        first, second = conv[0, here, :].astype(f32), conv[1, here, :].astype(f32)
        count = 2 * local
        mean = (
            jnp.sum(first, axis=-1, keepdims=True) + jnp.sum(second, axis=-1, keepdims=True)
        ) / count
        first, second = first - mean, second - mean
        var = (
            jnp.sum(first * first, axis=-1, keepdims=True)
            + jnp.sum(second * second, axis=-1, keepdims=True)
        ) / count
        scale = lax.rsqrt(var + eps)
        first = first * scale * gain_ref[:, :local]
        second = second * scale * gain_ref[:, local:]
        first = (first * jax.nn.sigmoid(first)).astype(bf16)
        second = (second * jax.nn.sigmoid(second)).astype(bf16)
        mixer_ref[here, :] = (_dot(first, wo[:local, :]) + _dot(second, wo[local:, :])).astype(bf16)

    def combine(k):
        return acc[...] + weighed(k, results[peers[k]])

    def returned(k, n):
        for s in range(subs):
            back_copy(k, s, n, peers[k]).wait_recv()

    send_far()
    for k in near:
        rows_k = [_dot(pickers[k], normed[h]).astype(bf16) for h in range(2)]
        for h in range(2):
            for s in range(subs):
                picked[k, h, s] = rows_k[h][cut(s)]
        near_dispatch(k, z).start()
    for h in range(2):
        rows_0 = _dot(pickers[0], normed[h]).astype(bf16)
        for s in range(subs):
            block[z, h, s, c] = rows_0[cut(s)]
    core_copies(0, c).start()
    kept = slice(0, length - halo)
    for i in range(cols):
        at = slice(i * LANES, (i + 1) * LANES)
        gated = value_ref[kept, at].astype(f32) * jax.nn.sigmoid(gate_ref[kept, at].astype(f32))
        glu[i, halo:length, :] = gated.astype(bf16).astype(f32)
        glu[i, length:, :] = halo_out[:, at].astype(f32)
    if not convolve(1, early, True):
        gather(0, early - 1)
    convolve(early, pieces)
    mid_far, last_far = far[:-1], far[-1]
    units = [(k, s) for k in mid_far for s in range(subs)]
    lane = _iota((tokens, LANES), 1)
    index = _iota((8, tokens), 0)
    rows_named = jnp.where(index == 0, r0t, 0).astype(f32) + jnp.where(index == 1, r1t, 0).astype(f32)
    for j in range(2):
        rows_named = rows_named + jnp.where(index == 2 + j, rw_t_ref[j : j + 1, :], 0.0)
    named = jnp.transpose(rows_named)
    r0, r1 = (named[:, j : j + 1].astype(jnp.int32) for j in range(2))
    hits = ((r0 == lane) | (r1 == lane)).astype(f32).astype(bf16)
    earlier = (_iota((tokens, tokens), 1) < _iota((tokens, tokens), 0)).astype(f32).astype(bf16)
    place = _dot(earlier, hits)
    slot_of = _iota((tokens, cap), 1)
    places = [
        jnp.sum(jnp.where(lane == r, place, 0.0), axis=1, keepdims=True).astype(jnp.int32)
        for r in (r0, r1)
    ]
    for k in range(chips):
        comb = jnp.zeros((tokens, cap), f32)
        for j, r in enumerate((r0, r1)):
            mine = jnp.where(r == peers[k], places[j], -1)
            comb = comb + jnp.where(slot_of == mine, named[:, 2 + j : 3 + j], 0.0)
        head = comb.astype(bf16)
        combs[k, 0] = head
        combs[k, 1] = (comb - head.astype(f32)).astype(bf16)


    halo_copy.wait_recv()
    before = jnp.where(ep > 0, halo_in[...].astype(f32), 0.0)
    for i in range(cols):
        glu[i, :halo, :] = before[:, i * LANES : (i + 1) * LANES]
    convolve(0, 1)
    for copy in weights[:3]:
        copy.wait()
    from_cores(0)
    feed_forward(0, 0, cap, lambda: far_in(*units[0]))
    later = min(len(groups), early)
    gather(early - 1, later)
    far_over(*units[0])
    for unit in units[1:]:
        far_in(*unit)
    for o in range(2):
        near_sum(0, o)
    for h in range(2):
        from_core(units[0][0], h, units[0][1])
    feed_forward(*units[0], few, lambda: far_in(last_far, 0))

    def near_ins():
        for k in near:
            near_in(k)

    def last_ins():
        for s in range(1, subs):
            far_in(last_far, s)

    if len(units) == 1:
        near_ins()
        last_ins()
    for i in range(1, len(units)):
        far_over(*units[i])
        pair_sum(*units[i - 1], few)
        for h in range(2):
            from_core(units[i][0], h, units[i][1])
        only = i == 1
        feed_forward(*units[i], few, near_ins if only else None, last_ins if only else None)
    far_over(last_far, 0)
    for k in near:
        from_cores(k)

    def first_back():
        pair_sum(*units[-1], few)
        plane_sum(*units[0], few)

    for k in near:
        feed_forward(k, 0, cap, first_back if k == near[0] else None)
    gather(later, len(groups) - 1)
    for s in range(1, subs):
        far_over(last_far, s)

    def near_sums(o):
        for k in near:
            near_sum(k, o)


    for s in range(subs):
        for h in range(2):
            from_core(last_far, h, s)
        if s == 0:
            feed_forward(last_far, s, few, lambda: near_sums(0), lambda: near_sums(1))
        else:
            for unit in units[1:] if s == 1 else []:
                plane_sum(*unit, few)
            feed_forward(last_far, s, few, lambda: pair_sum(last_far, s - 1, few))
    pair_sum(last_far, subs - 1, few)
    gather(len(groups) - 1, len(groups))
    weights[3].wait()
    group = 2 if pieces % 2 == 0 else 1
    mix(group, 2 * group)
    plane_sum(last_far, 0, few)
    for p in range(2 * group, pieces, group):
        mix(p, p + group)

    def lend_all():
        lend(0)
        lend(1)

    pl.when(swap == 0)(lend_all)
    pl.when(swap == 1)(lambda: lend(0))
    for s in range(1, subs):
        plane_sum(last_far, s, few)
    pl.when(swap == 1)(lambda: lend(1))
    mix(0, group)
    keep()
    for k in far[:-1]:
        returned(k, few)
        acc[...] = combine(k)
    for j in range(2):
        q_copy(j).wait_recv()
    acc[...] = acc[...] + q_in[...].astype(f32)
    returned(far[-1], few)
    routed_ref[...] = combine(far[-1]).astype(bf16)

    half = block.at[pl.ds(0, chips // 2)]
    for name, ref in (
        ("disp", block.at[0]),
        ("core", half),
        ("pair", half),
        ("cross", block.at[0]),
        ("back", block.at[0]),
        ("ag", conv.at[0]),
        ("q", q_out),
        ("halo", halo_out),
    ):
        remote(ref, ref, to_send[name], halo_recv.at[0], core_peer).wait_send()


def store_kernel(mixer_ref, routed_ref, mixer_hbm, routed_hbm, sem):
    copies = [
        pltpu.make_async_copy(mixer_ref, mixer_hbm, sem.at[0]),
        pltpu.make_async_copy(routed_ref, routed_hbm, sem.at[1]),
    ]
    for copy in copies:
        copy.start()
    for copy in copies:
        copy.wait()


def one_kernel(
    value_in,
    gate_in,
    conv_taps,
    chan_gain,
    out_weight,
    second_rows,
    expert_gain,
    routes,
    route_weights,
    gate_w,
    up_w,
    down_w,
):
    chips = lax.axis_size("ep") // 2
    tokens, model = second_rows.shape
    top = routes.shape[1]
    width = model // 2
    cap = 2 * max(1, min(tokens // 2, 3 * tokens * top // (4 * chips)))
    subs = 2 if cap % 32 == 0 else 1
    few = cap // subs
    length, local = value_in.shape
    units = gate_w.shape[2]
    halo = -(-(conv_taps.shape[0] - 1) // 16) * 16
    pieces = 8 if length % 128 == 0 and length // 8 > halo else 1
    bf16, f32 = jnp.bfloat16, jnp.float32
    vmem = pl.BlockSpec(memory_space=pltpu.VMEM)
    hbm = pl.BlockSpec(memory_space=pltpu.HBM)
    dma = pltpu.SemaphoreType.DMA
    scratch = [
        pltpu.VMEM(value_in.shape, bf16),
        pltpu.VMEM(gate_in.shape, bf16),
        pltpu.VMEM(conv_taps.shape, f32),
        pltpu.VMEM((1, chan_gain.shape[0]), f32),
        pltpu.VMEM(second_rows.shape, bf16),
        pltpu.VMEM((1, model), f32),
        pltpu.VMEM((top, tokens), jnp.int32),
        pltpu.VMEM((top, tokens), f32),
        pltpu.VMEM(out_weight.shape, bf16),
        pltpu.VMEM(gate_w.shape[1:], bf16),
        pltpu.VMEM(up_w.shape[1:], bf16),
        pltpu.VMEM(down_w.shape[1:], bf16),
        pltpu.VMEM((2, tokens, width), bf16),
        pltpu.VMEM((chips, 2, subs, few, width), bf16),
        pltpu.VMEM((chips, 2, subs, 2, few, width), bf16),
        pltpu.VMEM((2 * cap, units), bf16),
        pltpu.VMEM((chips, 2, 2, cap, width), bf16),
        pltpu.VMEM((chips, 2, cap, width), bf16),
        pltpu.VMEM((chips, cap, width), bf16),
        pltpu.VMEM((chips, cap, width), bf16),
        pltpu.VMEM((chips, cap, width), bf16),
        pltpu.VMEM((chips, cap, width), bf16),
        pltpu.VMEM((chips // 2, 2, cap, width), bf16),
        pltpu.VMEM((chips // 2, 2, cap, width), bf16),
        pltpu.VMEM((tokens, width), bf16),
        pltpu.VMEM((tokens, width), bf16),
        pltpu.VMEM((chips, 2, tokens, cap), bf16),
        pltpu.VMEM((tokens, width), f32),
        pltpu.VMEM((local // LANES, halo + length, LANES), f32),
        pltpu.VMEM((halo, local), bf16),
        pltpu.VMEM((halo, local), bf16),
        pltpu.VMEM((2, length, local), bf16),
        dma((4,)),
        dma((8,)),
        dma((chips // 2, subs)),
        dma((chips // 2 - 1,)),
        dma((chips // 2, subs)),
        dma((chips // 2, 2, subs)),
        dma((chips // 2,)),
        dma((chips // 2 + chips // 2 * subs, 2)),
        dma((chips // 2, subs)),
        dma((chips // 2, subs)),
        dma((chips // 2 - 1, 3)),
        dma((2,)),
        dma((min(pieces, 4) + (pieces - min(pieces, 4) + 1) // 2,)),
        dma((1,)),
        dma((8,)),
    ]
    outs = pl.pallas_call(
        functools.partial(step_kernel, chips, cap, subs, pieces, halo),
        out_shape=(
            jax.ShapeDtypeStruct((length, out_weight.shape[1]), bf16),
            jax.ShapeDtypeStruct((tokens, width), bf16),
        ),
        in_specs=[hbm] * 12,
        out_specs=(vmem, vmem),
        scratch_shapes=scratch,
        compiler_params=pltpu.CompilerParams(
            collective_id=0, has_side_effects=True, vmem_limit_bytes=40 * 1024 * 1024
        ),
    )(
        *(
            pltpu.with_memory_space_constraint(value, pltpu.HBM)
            for value in (
                value_in,
                gate_in,
                conv_taps,
                chan_gain.reshape(1, -1),
                out_weight,
                second_rows,
                expert_gain.reshape(1, -1),
                routes.T,
                route_weights.T,
                gate_w,
                up_w,
                down_w,
            )
        )
    )
    return pl.pallas_call(
        store_kernel,
        out_shape=tuple(jax.ShapeDtypeStruct(out.shape, out.dtype) for out in outs),
        in_specs=[vmem] * 2,
        out_specs=(pl.BlockSpec(memory_space=pl.ANY),) * 2,
        scratch_shapes=[dma((2,))],
        compiler_params=pltpu.CompilerParams(vmem_limit_bytes=1024 * 1024),
    )(*outs)


def solution(mesh):
    chips = mesh.shape["ep"] // 2
    paired = mesh.shape["tp"] == 2 and chips == 4
    placed = (
        P(("grp", "ep"), "tp"),
        P(("grp", "ep"), "tp"),
        P(None, "tp"),
        P(),
        P(None, "tp"),
        P(("grp", "ep"), None),
        P(),
        P(("grp", "ep"), None),
        P(("grp", "ep"), None),
        P("ep", None, "tp"),
        P("ep", None, "tp"),
        P("ep", "tp", None),
    )
    return jax.shard_map(
        one_kernel if paired else on_device,
        mesh=mesh,
        in_specs=placed,
        out_specs=(P(("grp", "ep"), "tp"), P(("grp", "ep"), "tp")),
        check_vma=False,
    )
```
